32 devices in a mesh: sp: 16 (over z, y, x), tp: 2 (over core).
Axes of the slice: x: 2, y: 2, z: 4, core: 2. Of those that a mesh axis runs over, the one named last changes fastest.
Arguments:
- tokens: bfloat16 [8192, 2048], P('sp', 'tp'), may hold values from -6 to 6
- norm_gain: float32 [2048], replicated, may hold values from 0.1 to 1.9
- outer_gate: bfloat16 [2048, 1024], P('sp', 'tp'), may hold values from -0.125 to 0.125
- inner_gate: bfloat16 [2048, 1024], P('sp', 'tp'), may hold values from -0.125 to 0.125
- conv_input: bfloat16 [2048, 1024], P('sp', 'tp'), may hold values from -0.125 to 0.125
- query_proj: bfloat16 [2048, 1024], P('sp', 'tp'), may hold values from -0.125 to 0.125
- key_proj: bfloat16 [2048, 1024], P('sp', 'tp'), may hold values from -0.125 to 0.125
- value_proj: bfloat16 [2048, 1024], P('sp', 'tp'), may hold values from -0.125 to 0.125
- out_gate: bfloat16 [2048, 1024], P('sp', 'tp'), may hold values from -0.125 to 0.125
- conv_taps: float32 [3, 1024], P(None, 'tp'), may hold values from -3.5 to 3.5
- log_decay: float32 [2, 16, 8192], P(None, 'tp', 'sp'), may hold values from -1.2 to 0, as said below
- head_gain: float32 [1024], P('tp'), may hold values from 0.1 to 1.9
- conv_output: bfloat16 [1024, 2048], P('tp', 'sp'), may hold values from -0.1875 to 0.1875
- retention_output: bfloat16 [1024, 2048], P('tp', 'sp'), may hold values from -0.1875 to 0.1875
Outputs:
- mixed: bfloat16 [8192, 2048], P(('sp', 'tp'))
The draws below stay inside these ranges and needn't reach their ends.
Inputs may be any that keep to these rules, and one draw needn't show every extreme that they name: `log_decay`: logarithms of per-position decays, below zero.
All inputs are finite; a program needn't handle non-finite values.
Results may differ from the reference program's by a relative error of at most 0.02.
Values may be sent and summed in bfloat16 or wider, within the bound.
A program may use at most 128 MiB of HBM per device.

```python
import math
import jax
import jax.numpy as jnp
from jax import lax

D = 2048
CONV_CH = 1024
HEAD_NUMBER = 16
HEAD_DIM = 64
TOK_DEV = 512
TOKEN_NUMBER = 8192
N_SP = 16
N_TP = 2


def draw_log_decay(key, part):
    key_sequence = jax.random.split(jax.random.fold_in(key, 17), 6)
    span_count = TOKEN_NUMBER // TOK_DEV
    is_fast = jax.random.uniform(key_sequence[0], (2, HEAD_NUMBER, 1), jnp.float32) < 0.5
    fast_rate = jax.random.uniform(key_sequence[1], (2, HEAD_NUMBER, 1), jnp.float32, 0.01, 0.02)
    slow_rate = jax.random.uniform(key_sequence[2], (2, HEAD_NUMBER, 1), jnp.float32, 0.1, 0.3) / TOKEN_NUMBER
    selected_rate = jnp.where(is_fast, fast_rate, slow_rate)
    multiplier = jnp.exp(jax.random.uniform(key_sequence[3], (2, HEAD_NUMBER, span_count), jnp.float32, 0.0, math.log(4.0)))
    multiplier = jnp.repeat(multiplier, TOK_DEV, axis=2)
    flurry_location = jax.random.randint(key_sequence[4], (2, HEAD_NUMBER, 2, 1), 0, TOKEN_NUMBER)
    flurry_depth = jax.random.uniform(key_sequence[5], (2, HEAD_NUMBER, 2, 1), jnp.float32, 0.22, 0.51)
    position_list = jnp.arange(TOKEN_NUMBER, dtype=jnp.int32)
    flurry_list = jnp.sum(jnp.where(position_list == flurry_location, flurry_depth, 0.0), axis=2)
    return (-(selected_rate * multiplier) - flurry_list).astype(jnp.float32)


def shard_levels(stream_key, dims, pieces, least, largest):
    gain, own = 1.0, jax.random.fold_in(stream_key, 6)
    for axis_at, blocks in pieces:
        steps = jnp.exp(jax.random.uniform(jax.random.fold_in(own, axis_at), (blocks,), jnp.float32, least / len(pieces), largest / len(pieces)))
        gain = gain * jnp.repeat(steps, dims[axis_at] // blocks).reshape([-1 if axis == axis_at else 1 for axis in range(len(dims))])
    return gain


def centred(stream_key, dims, width, reach, cuts=(), held_as=jnp.bfloat16):
    gain = shard_levels(stream_key, dims, cuts, -0.22, 0.18) if cuts else 1.0
    entries = jax.random.normal(stream_key, dims, jnp.float32) * width * gain
    return jnp.minimum(jnp.maximum(entries, -reach), reach).astype(held_as)


def setup_inputs(seed: int = 0) -> dict:
    seeds = jax.random.split(jax.random.key(seed), 15)
    tokens = centred(seeds[0], (TOKEN_NUMBER, D), 1.0, 6.0, ((0, 16), (1, 2)))
    norm_gain = jnp.clip(1.0 + 0.18 * jax.random.normal(seeds[1], (D,), jnp.float32), 0.1, 1.9)
    outer_gate = centred(seeds[2], (D, CONV_CH), D ** -0.5, 0.125, ((0, 16), (1, 2)))
    inner_gate = centred(seeds[3], (D, CONV_CH), D ** -0.5, 0.125, ((0, 16), (1, 2)))
    conv_input = centred(seeds[4], (D, CONV_CH), D ** -0.5, 0.125, ((0, 16), (1, 2)))
    query_proj = centred(seeds[5], (D, HEAD_NUMBER * HEAD_DIM), D ** -0.5, 0.125, ((0, 16), (1, 2)))
    key_proj = centred(seeds[6], (D, HEAD_NUMBER * HEAD_DIM), D ** -0.5, 0.125, ((0, 16), (1, 2)))
    value_proj = centred(seeds[7], (D, HEAD_NUMBER * HEAD_DIM), D ** -0.5, 0.125, ((0, 16), (1, 2)))
    out_gate = centred(seeds[8], (D, HEAD_NUMBER * HEAD_DIM), D ** -0.5, 0.125, ((0, 16), (1, 2)))
    conv_taps = centred(seeds[9], (3, CONV_CH), 3 ** -0.5, 3.5, ((1, 2),), jnp.float32)
    log_decay = draw_log_decay(jax.random.fold_in(seeds[14], 71), 0)
    head_gain = jnp.clip(1.0 + 0.18 * jax.random.normal(seeds[11], (HEAD_NUMBER * HEAD_DIM,), jnp.float32), 0.1, 1.9)
    conv_output = centred(seeds[12], (CONV_CH, D), CONV_CH ** -0.5, 0.1875, ((0, 2), (1, 16)))
    retention_output = centred(seeds[13], (HEAD_NUMBER * HEAD_DIM, D), (HEAD_NUMBER * HEAD_DIM) ** -0.5, 0.1875, ((0, 2), (1, 16)))
    return {"tokens": tokens, "norm_gain": norm_gain, "outer_gate": outer_gate, "inner_gate": inner_gate, "conv_input": conv_input, "query_proj": query_proj, "key_proj": key_proj, "value_proj": value_proj, "out_gate": out_gate, "conv_taps": conv_taps, "log_decay": log_decay, "head_gain": head_gain, "conv_output": conv_output, "retention_output": retention_output}


EPS = 1e-06
THETA = 10000.0

def rounded(array):
    return lax.optimization_barrier(array.astype(jnp.bfloat16)).astype(jnp.float32)

def rotate(field_in, position_list):
    half_dim = field_in.shape[-1] // 2
    frequency = jnp.exp(-jnp.log(THETA) * jnp.arange(half_dim, dtype=jnp.float32) * (2.0 / field_in.shape[-1]))
    angles = position_list.astype(jnp.float32)[:, None, None] * frequency
    cosine = jnp.cos(angles)
    sine_part = jnp.sin(angles)
    leading = field_in[..., :half_dim]
    trailing = field_in[..., half_dim:]
    return jnp.concatenate([leading * cosine - trailing * sine_part, leading * sine_part + trailing * cosine], axis=-1)

def span_parts(query_rows, key_rows, value_rows, log_rates):
    length = query_rows.shape[0]
    forward_cum = jnp.cumsum(log_rates[0], axis=-1)
    backward_cum = jnp.flip(jnp.cumsum(jnp.flip(log_rates[1], -1), axis=-1), -1)
    row_index = lax.broadcasted_iota(jnp.int32, (length, length), 0)
    col_index = lax.broadcasted_iota(jnp.int32, (length, length), 1)
    lower_part = (col_index <= row_index)[None]
    spread = jnp.where(lower_part, forward_cum[:, :, None] - forward_cum[:, None, :], backward_cum[:, :, None] - backward_cum[:, None, :])
    scores = jnp.einsum('ihe,jhe->hij', query_rows.astype(jnp.float32), key_rows.astype(jnp.float32))
    weighted = rounded(scores * jnp.exp(spread))
    local_part = jnp.einsum('hij,jhe->ihe', weighted, value_rows.astype(jnp.float32))
    key_wide = key_rows.astype(jnp.float32)
    forward_keys = rounded(key_wide * jnp.exp(forward_cum[:, -1:] - forward_cum).T[:, :, None])
    backward_keys = rounded(key_wide * jnp.exp(backward_cum[:, :1] - backward_cum).T[:, :, None])
    forward_state = jnp.einsum('jhd,jhe->hde', forward_keys, value_rows.astype(jnp.float32))
    backward_state = jnp.einsum('jhd,jhe->hde', backward_keys, value_rows.astype(jnp.float32))
    return (local_part, forward_cum, backward_cum, forward_state, backward_state)

def span_item(inputs):
    return span_parts(inputs[0], inputs[1], inputs[2], inputs[3])

def carried(query_rows, forward_cum, backward_cum, into_forward, into_backward):
    query_wide = query_rows.astype(jnp.float32)
    forward_part = jnp.einsum('ihd,hde->ihe', query_wide, rounded(into_forward))
    backward_part = jnp.einsum('ihd,hde->ihe', query_wide, rounded(into_backward))
    return jnp.exp(forward_cum).T[:, :, None] * forward_part + jnp.exp(backward_cum).T[:, :, None] * backward_part

def finish(mixed_heads, gate_rows, head_gain):
    row_count, head_count, head_width = mixed_heads.shape
    scaled = mixed_heads * lax.rsqrt(lax.optimization_barrier(jnp.mean(mixed_heads * mixed_heads, axis=-1, keepdims=True)) + EPS)
    scaled = scaled * head_gain.reshape(head_count, head_width)
    return (jax.nn.silu(gate_rows.astype(jnp.float32)) * scaled.reshape(row_count, head_count * head_width)).astype(jnp.bfloat16)

def forward_step(running, inputs):
    return (jnp.exp(inputs[0])[:, None, None] * running + inputs[1], running)

def reference(tokens, norm_gain, outer_gate, inner_gate, conv_input, query_proj, key_proj, value_proj, out_gate, conv_taps, log_decay, head_gain, conv_output, retention_output):
    wide = tokens.astype(jnp.float32)
    normed = (wide * lax.rsqrt(lax.optimization_barrier(jnp.mean(wide * wide, axis=-1, keepdims=True)) + EPS) * norm_gain).astype(jnp.bfloat16)
    projected = [jnp.dot(normed, weight, preferred_element_type=jnp.float32).astype(jnp.bfloat16) for weight in (outer_gate, inner_gate, conv_input, query_proj, key_proj, value_proj, out_gate)]
    inner_value = (projected[1].astype(jnp.float32) * projected[2].astype(jnp.float32)).astype(jnp.bfloat16)
    padded = jnp.pad(inner_value.astype(jnp.float32), ((1, 1), (0, 0)))
    convolved = conv_taps[0] * padded[:-2] + conv_taps[1] * padded[1:-1] + conv_taps[2] * padded[2:]
    conv_out = (projected[0].astype(jnp.float32) * convolved).astype(jnp.bfloat16)
    position_list = jnp.arange(TOKEN_NUMBER, dtype=jnp.int32)
    shape_heads = (TOKEN_NUMBER, HEAD_NUMBER, HEAD_DIM)
    rotated_query = rotate(projected[3].astype(jnp.float32).reshape(shape_heads), position_list).astype(jnp.bfloat16)
    rotated_key = (rotate(projected[4].astype(jnp.float32).reshape(shape_heads), position_list) * HEAD_DIM ** (-0.5)).astype(jnp.bfloat16)
    value_heads = projected[5].reshape(shape_heads)
    span_shape = (N_SP, TOK_DEV, HEAD_NUMBER, HEAD_DIM)
    span_rates = log_decay.reshape(2, HEAD_NUMBER, N_SP, TOK_DEV).transpose(2, 0, 1, 3)
    span_query = rotated_query.reshape(span_shape)
    local_part, forward_cum, backward_cum, forward_state, backward_state = lax.map(span_item, (span_query, rotated_key.reshape(span_shape), value_heads.reshape(span_shape), span_rates))
    blank = jnp.zeros((HEAD_NUMBER, HEAD_DIM, HEAD_DIM), jnp.float32)
    into_forward = lax.scan(forward_step, blank, (forward_cum[:, :, -1], forward_state))[1]
    into_backward = lax.scan(forward_step, blank, (backward_cum[:, :, 0], backward_state), reverse=True)[1]
    carried_part = jax.vmap(carried)(span_query, forward_cum, backward_cum, into_forward, into_backward)
    mixed_heads = (local_part + carried_part).reshape(shape_heads)
    ret_out = finish(mixed_heads, projected[6], head_gain)
    conv_group = CONV_CH // N_TP
    ret_group = HEAD_NUMBER * HEAD_DIM // N_TP
    total_sum = jnp.zeros((TOKEN_NUMBER, D), jnp.float32)
    for group_index in range(N_TP):
        conv_lo = group_index * conv_group
        ret_lo = group_index * ret_group
        partial_sum = jnp.dot(conv_out[:, conv_lo:conv_lo + conv_group], conv_output[conv_lo:conv_lo + conv_group], preferred_element_type=jnp.float32)
        partial_sum = partial_sum + jnp.dot(ret_out[:, ret_lo:ret_lo + ret_group], retention_output[ret_lo:ret_lo + ret_group], preferred_element_type=jnp.float32)
        total_sum = total_sum + rounded(partial_sum)
    return total_sum.astype(jnp.bfloat16)
```

```python
import jax
import jax.numpy as jnp
from jax import lax
from jax.sharding import PartitionSpec as P

HEAD_DIM = 64


EPS = 1e-06
THETA = 10000.0


def with_halo(shard, sides, width):
    for axis, dim in sides:
        size, length = (lax.axis_size(axis), shard.shape[dim])
        up = [(i, (i + 1) % size) for i in range(size - 1)]
        down = [(j, i) for i, j in up]
        last = lax.slice_in_dim(shard, length - width, length, axis=dim)
        first = lax.slice_in_dim(shard, 0, width, axis=dim)
        before = lax.ppermute(last, axis, up)
        after = lax.ppermute(first, axis, down)
        shard = jnp.concatenate([before, shard, after], axis=dim)
    return shard


def rotate(field_in, position_list):
    half_dim = field_in.shape[-1] // 2
    frequency = jnp.exp(
        -jnp.log(THETA) * jnp.arange(half_dim, dtype=jnp.float32) * (2.0 / field_in.shape[-1])
    )
    angles = position_list.astype(jnp.float32)[:, None, None] * frequency
    cosine = jnp.cos(angles)
    sine_part = jnp.sin(angles)
    leading = field_in[..., :half_dim]
    trailing = field_in[..., half_dim:]
    return jnp.concatenate(
        [leading * cosine - trailing * sine_part, leading * sine_part + trailing * cosine], axis=-1
    )


def conv_branch(outer_rows, inner_rows, conv_values, conv_taps):
    inner_value = (inner_rows.astype(jnp.float32) * conv_values.astype(jnp.float32)).astype(
        jnp.bfloat16
    )
    padded = with_halo(inner_value, (("sp", 0),), 1).astype(jnp.float32)
    convolved = conv_taps[0] * padded[:-2] + conv_taps[1] * padded[1:-1] + conv_taps[2] * padded[2:]
    return (outer_rows.astype(jnp.float32) * convolved).astype(jnp.bfloat16)


def span_parts(query_rows, key_rows, value_rows, log_rates):
    length = query_rows.shape[0]
    forward_cum = jnp.cumsum(log_rates[0], axis=-1)
    backward_cum = jnp.flip(jnp.cumsum(jnp.flip(log_rates[1], -1), axis=-1), -1)
    row_index = lax.broadcasted_iota(jnp.int32, (length, length), 0)
    col_index = lax.broadcasted_iota(jnp.int32, (length, length), 1)
    lower_part = (col_index <= row_index)[None]
    spread = jnp.where(
        lower_part,
        forward_cum[:, :, None] - forward_cum[:, None, :],
        backward_cum[:, :, None] - backward_cum[:, None, :],
    )
    scores = jnp.einsum("ihe,jhe->hij", query_rows, key_rows, preferred_element_type=jnp.float32)
    weighted = (scores * jnp.exp(spread)).astype(jnp.bfloat16)
    local_part = jnp.einsum(
        "hij,jhe->ihe", weighted, value_rows, preferred_element_type=jnp.float32
    )
    key_wide = key_rows.astype(jnp.float32)
    forward_keys = (key_wide * jnp.exp(forward_cum[:, -1:] - forward_cum).T[:, :, None]).astype(
        jnp.bfloat16
    )
    backward_keys = (key_wide * jnp.exp(backward_cum[:, :1] - backward_cum).T[:, :, None]).astype(
        jnp.bfloat16
    )
    forward_state = jnp.einsum(
        "jhd,jhe->hde", forward_keys, value_rows, preferred_element_type=jnp.float32
    )
    backward_state = jnp.einsum(
        "jhd,jhe->hde", backward_keys, value_rows, preferred_element_type=jnp.float32
    )
    return (local_part, forward_cum, backward_cum, forward_state, backward_state)


def retention_branch(query_rows, key_rows, value_rows, gate_rows, log_decay, head_gain, offsets):
    row_count = query_rows.shape[0]
    head_count = query_rows.shape[1] // HEAD_DIM
    shape_heads = (row_count, head_count, HEAD_DIM)
    rotated_query = rotate(query_rows.astype(jnp.float32).reshape(shape_heads), offsets).astype(
        jnp.bfloat16
    )
    rotated_key = (
        rotate(key_rows.astype(jnp.float32).reshape(shape_heads), offsets) * HEAD_DIM ** (-0.5)
    ).astype(jnp.bfloat16)
    local_part, forward_cum, backward_cum, forward_state, backward_state = span_parts(
        rotated_query, rotated_key, value_rows.reshape(shape_heads), log_decay
    )
    forward_total = forward_cum[:, -1]
    backward_total = backward_cum[:, 0]
    totals = lax.all_gather(
        jnp.stack([forward_total, backward_total])[None], "sp", axis=0, tiled=True
    )
    inclusive = jnp.cumsum(totals, axis=0)
    exclusive = inclusive - totals
    own_index = lax.axis_index("sp")
    own_inclusive = lax.dynamic_index_in_dim(inclusive, own_index, 0, keepdims=False)
    own_exclusive = lax.dynamic_index_in_dim(exclusive, own_index, 0, keepdims=False)
    pieces = (
        lax.all_gather(forward_state[None], "sp", axis=0, tiled=True),
        lax.all_gather(backward_state[None], "sp", axis=0, tiled=True),
    )
    piece_count = pieces[0].shape[0]
    span_index = lax.iota(jnp.int32, piece_count)
    forward_weight = jnp.where(
        (span_index < own_index)[:, None],
        jnp.exp(jnp.minimum(own_exclusive[0] - inclusive[:, 0], 0.0)),
        0.0,
    )
    backward_weight = jnp.where(
        (span_index > own_index)[:, None],
        jnp.exp(jnp.minimum(exclusive[:, 1] - own_inclusive[1], 0.0)),
        0.0,
    )
    into_forward = jnp.einsum(
        "nh,nhde->hde", forward_weight, pieces[0], precision=lax.Precision.HIGHEST
    )
    into_backward = jnp.einsum(
        "nh,nhde->hde", backward_weight, pieces[1], precision=lax.Precision.HIGHEST
    )
    forward_part = jnp.einsum(
        "ihd,hde->ihe",
        rotated_query,
        into_forward.astype(jnp.bfloat16),
        preferred_element_type=jnp.float32,
    )
    backward_part = jnp.einsum(
        "ihd,hde->ihe",
        rotated_query,
        into_backward.astype(jnp.bfloat16),
        preferred_element_type=jnp.float32,
    )
    mixed_heads = (
        local_part
        + jnp.exp(forward_cum).T[:, :, None] * forward_part
        + jnp.exp(backward_cum).T[:, :, None] * backward_part
    )
    scaled = mixed_heads * lax.rsqrt(
        jnp.mean(mixed_heads * mixed_heads, axis=-1, keepdims=True) + EPS
    )
    scaled = scaled * head_gain.reshape(head_count, HEAD_DIM)
    return (
        jax.nn.silu(gate_rows.astype(jnp.float32))
        * scaled.reshape(row_count, head_count * HEAD_DIM)
    ).astype(jnp.bfloat16)


def local(
    tokens,
    norm_gain,
    outer_gate,
    inner_gate,
    conv_input,
    query_proj,
    key_proj,
    value_proj,
    out_gate,
    conv_taps,
    log_decay,
    head_gain,
    conv_output,
    retention_output,
):
    whole = lax.all_gather(tokens, "tp", axis=1, tiled=True)
    wide = whole.astype(jnp.float32)
    normed = (
        wide * lax.rsqrt(jnp.mean(wide * wide, axis=-1, keepdims=True) + EPS) * norm_gain
    ).astype(jnp.bfloat16)
    row_count = normed.shape[0]
    offsets = lax.axis_index("sp") * row_count + lax.iota(jnp.int32, row_count)
    gathered = (
        lax.all_gather(outer_gate, "sp", axis=0, tiled=True),
        lax.all_gather(inner_gate, "sp", axis=0, tiled=True),
        lax.all_gather(conv_input, "sp", axis=0, tiled=True),
        lax.all_gather(query_proj, "sp", axis=0, tiled=True),
        lax.all_gather(key_proj, "sp", axis=0, tiled=True),
        lax.all_gather(value_proj, "sp", axis=0, tiled=True),
        lax.all_gather(out_gate, "sp", axis=0, tiled=True),
        lax.all_gather(conv_output, "sp", axis=1, tiled=True),
        lax.all_gather(retention_output, "sp", axis=1, tiled=True),
    )
    projected = [
        jnp.dot(normed, weight, preferred_element_type=jnp.float32).astype(jnp.bfloat16)
        for weight in gathered[:7]
    ]
    conv_out = conv_branch(projected[0], projected[1], projected[2], conv_taps)
    ret_out = retention_branch(
        projected[3], projected[4], projected[5], projected[6], log_decay, head_gain, offsets
    )
    conv_weight = gathered[7]
    ret_weight = gathered[8]
    return lax.psum_scatter(
        (
            jnp.dot(conv_out, conv_weight, preferred_element_type=jnp.float32)
            + jnp.dot(ret_out, ret_weight, preferred_element_type=jnp.float32)
        ).astype(jnp.bfloat16),
        "tp",
        scatter_dimension=0,
        tiled=True,
    )


def plane_local(planes, group, arrays):
    (
        tokens,
        norm_gain,
        outer_gate,
        inner_gate,
        conv_input,
        query_proj,
        key_proj,
        value_proj,
        out_gate,
        conv_taps,
        log_decay,
        head_gain,
        conv_output,
        retention_output,
    ) = arrays
    spans = planes * group
    own = lax.axis_index("sp")
    core = lax.axis_index("tp")
    place = lax.rem(own, group)
    plane = lax.div(own, group)
    length, half_width = tokens.shape
    width = half_width * 2
    channels = outer_gate.shape[1] // group
    heads = channels // HEAD_DIM
    f32, bf16 = jnp.float32, jnp.bfloat16

    def swap(x, d):
        return lax.ppermute(x, "sp", [(i, i ^ d) for i in range(spans)])

    def up(x, k=1):
        return lax.ppermute(x, "sp", [(i, i + k * group) for i in range(spans - k * group)])

    def down(x, k=1):
        return lax.ppermute(x, "sp", [(i + k * group, i) for i in range(spans - k * group)])

    def cross(x):
        return lax.ppermute(x, "tp", [(0, 1), (1, 0)])

    def pick(x, index, axis=0):
        return lax.dynamic_index_in_dim(x, index, axis, keepdims=False)

    def reorder(pieces):
        stacked = jnp.stack(pieces) if isinstance(pieces, (list, tuple)) else pieces
        return jnp.stack([pick(stacked, jnp.bitwise_xor(place, t)) for t in range(group)])

    def exchange(x, axis):
        return [pick(x, place, axis)] + [
            swap(pick(x, jnp.bitwise_xor(place, d), axis), d) for d in range(1, group)
        ]

    def along(x):
        ups, downs = [x], [x]
        for _ in range(planes - 1):
            ups.append(up(ups[-1]))
            downs.append(down(downs[-1]))
        rest = [
            jnp.where(plane + o < planes, downs[o], ups[planes - o]) for o in range(1, planes)
        ]
        return jnp.stack([x] + rest)

    def of_plane(stacked, t):
        return pick(stacked, lax.rem(t - plane + planes, planes))

    wide = tokens.astype(f32)
    square_sum = jnp.sum(wide * wide, axis=-1).reshape(-1, 128)
    square_sum = (square_sum + cross(square_sum)).reshape(length, 1)
    own_gain = lax.dynamic_slice_in_dim(norm_gain, core * half_width, half_width)
    normed = (wide * lax.rsqrt(square_sum / width + EPS) * own_gain).astype(bf16)

    def columns(weights):
        rows = weights[0].shape[0]
        stacked = jnp.stack([w.reshape(rows, group, channels) for w in weights], axis=2)
        stacked = stacked.reshape(rows, group, len(weights) * channels)
        block = reorder(exchange(stacked, 1))
        return block.reshape(group * rows, len(weights) * channels)

    retained = along(columns((key_proj, query_proj, value_proj)))
    others = along(columns((inner_gate, conv_input, outer_gate, out_gate)))
    out_cols = conv_output.shape[1]
    out_stack = jnp.concatenate(
        [w.reshape(group, channels, out_cols) for w in (conv_output, retention_output)], axis=1
    )
    out_block = reorder(exchange(out_stack, 0))
    out_block = out_block.transpose(1, 0, 2).reshape(2 * channels, group * out_cols)
    out_parts = along(out_block)

    rates = jnp.stack(
        exchange(log_decay.reshape(2, group, heads, length), 1)
    )

    quarter = half_width // 2
    first, second = normed[None, :, :quarter], normed[None, :, quarter:]
    first = jnp.concatenate([first, swap(first, 1)], axis=0)
    second = jnp.concatenate([second, swap(second, 2)], axis=0)
    first_far, second_far = swap(first, 2), swap(second, 1)
    first = jnp.concatenate([first, first_far], axis=0)
    second = jnp.stack([second[0], second_far[0], second[1], second_far[1]])
    rows_all = jnp.concatenate([first, second, cross(first), cross(second)], axis=-1)
    rows_all = rows_all.reshape(group * length, width)

    def project(stacked):
        order = (2 * core, 2 * core + 1, 2 * (1 - core), 2 * (1 - core) + 1)
        weight = jnp.concatenate([of_plane(stacked, t) for t in order], axis=0)
        return jnp.dot(rows_all, weight, preferred_element_type=f32).astype(bf16)

    span_ids = plane * group + jnp.bitwise_xor(place, lax.iota(jnp.int32, group))
    positions = (span_ids[:, None] * length + lax.iota(jnp.int32, length)).reshape(-1)
    half_dim = HEAD_DIM // 2
    frequency = jnp.exp(
        -jnp.log(THETA) * jnp.arange(half_dim, dtype=f32) * (2.0 / HEAD_DIM)
    )
    angles = positions.astype(f32)[:, None] * frequency
    cosine, sine = lax.optimization_barrier((jnp.cos(angles), jnp.sin(angles)))
    cosine, sine = cosine[:, None, :], sine[:, None, :]

    def turned(x):
        x = x.astype(f32).reshape(group * length, heads, HEAD_DIM)
        a, b = x[..., :half_dim], x[..., half_dim:]
        return jnp.concatenate([a * cosine - b * sine, a * sine + b * cosine], axis=-1)

    shape_heads = (group, length, heads, HEAD_DIM)
    kqv = project(retained)
    rk = (turned(kqv[:, :channels]) * HEAD_DIM ** (-0.5)).astype(bf16).reshape(shape_heads)
    rq = turned(kqv[:, channels : 2 * channels]).astype(bf16).reshape(shape_heads)
    value = kqv[:, 2 * channels :].reshape(shape_heads)
    local_part, forward_cum, backward_cum, forward_state, backward_state = jax.vmap(span_parts)(
        rq, rk, value, rates
    )
    forward_total = reorder(forward_cum[:, :, -1])
    backward_total = reorder(backward_cum[:, :, 0])
    forward_state = reorder(forward_state)
    backward_state = reorder(backward_state)

    def carry(states, totals, send):
        running = jnp.zeros_like(states[0])
        passed = jnp.zeros_like(totals[0])
        inside, reach = [], []
        for t in range(group):
            inside.append(running)
            reach.append(passed)
            running = jnp.exp(totals[t])[:, None, None] * running + states[t]
            passed = passed + totals[t]
        incoming, between = jnp.zeros_like(running), jnp.zeros_like(passed)
        for k in range(1, planes):
            incoming = incoming + jnp.exp(between)[:, None, None] * send(running, k)
            if k + 1 < planes:
                between = between + send(passed, k)
        return [
            a + jnp.exp(b)[:, None, None] * incoming for a, b in zip(inside, reach)
        ]

    into_forward = carry(list(forward_state), list(forward_total), up)
    into_backward = carry(list(backward_state)[::-1], list(backward_total)[::-1], down)[::-1]
    into_forward = reorder(into_forward).astype(bf16)
    into_backward = reorder(into_backward).astype(bf16)

    rest = project(others)
    inner_value = (
        rest[:, :channels].astype(f32) * rest[:, channels : 2 * channels].astype(f32)
    ).astype(bf16).reshape(group, length, channels)
    lasts = reorder(inner_value[:, -1:])
    firsts = reorder(inner_value[:, :1])
    before = reorder(jnp.concatenate([up(lasts[-1:]), lasts[:-1]], axis=0))
    after = reorder(jnp.concatenate([firsts[1:], down(firsts[:1])], axis=0))
    taps = lax.dynamic_slice_in_dim(conv_taps, place * channels, channels, axis=1)
    padded = jnp.concatenate([before, inner_value, after], axis=1).astype(f32)
    convolved = taps[0] * padded[:, :-2] + taps[1] * padded[:, 1:-1] + taps[2] * padded[:, 2:]
    outer = rest[:, 2 * channels : 3 * channels].reshape(group, length, channels)
    conv_out = (outer.astype(f32) * convolved).astype(bf16)

    forward_part = jnp.einsum("sihd,shde->sihe", rq, into_forward, preferred_element_type=f32)
    backward_part = jnp.einsum("sihd,shde->sihe", rq, into_backward, preferred_element_type=f32)
    mixed_heads = (
        local_part
        + jnp.exp(forward_cum).transpose(0, 2, 1)[..., None] * forward_part
        + jnp.exp(backward_cum).transpose(0, 2, 1)[..., None] * backward_part
    )
    scaled = mixed_heads * lax.rsqrt(
        jnp.mean(mixed_heads * mixed_heads, axis=-1, keepdims=True) + EPS
    )
    own_head_gain = lax.dynamic_slice_in_dim(head_gain, place * channels, channels)
    scaled = scaled.reshape(group, length, channels) * own_head_gain
    gate = rest[:, 3 * channels :].reshape(group, length, channels)
    ret_out = (jax.nn.silu(gate.astype(f32)) * scaled).astype(bf16)

    out_weight = jnp.concatenate([of_plane(out_parts, t) for t in range(planes)], axis=1)
    features = jnp.concatenate([conv_out, ret_out], axis=-1)
    features = features.reshape(group, 2, length // 2, 2 * channels)
    mine_rows, their_rows = pick(features, core, 1), pick(features, 1 - core, 1)
    half_out = out_weight.shape[1] // 2

    def partial(rows, ids, weight):
        picked = jnp.concatenate([rows[i] for i in ids], axis=0)
        return jnp.dot(picked, weight, preferred_element_type=f32)

    def chip_sum(ids, weight):
        theirs = cross(partial(their_rows, ids, weight).astype(bf16))
        total = partial(mine_rows, ids, weight) + theirs.astype(f32)
        return total.reshape(len(ids), length // 2, half_out)

    def scatter(weight, one, two):
        sent = swap(chip_sum((one, one ^ two), weight).astype(bf16), one)
        kept = chip_sum((0, two), weight) + sent.astype(f32)
        return kept[0] + swap(kept[1].astype(bf16), two).astype(f32)

    return jnp.concatenate(
        [
            scatter(out_weight[:, :half_out], 1, 2),
            scatter(out_weight[:, half_out:], 2, 1),
        ],
        axis=1,
    ).astype(bf16)


LANES = 128


def plan(*arrays):
    spans, cores = lax.axis_size("sp"), lax.axis_size("tp")
    group = arrays[2].shape[1] // LANES
    planes = spans // group
    fits = (
        cores == 2
        and group == 4
        and planes * group == spans
        and planes == 2 * cores
        and arrays[0].shape[1] == 2 * group * arrays[2].shape[0]
    )
    return plane_local(planes, group, arrays) if fits else local(*arrays)


def solution(mesh):
    return jax.shard_map(
        plan,
        mesh=mesh,
        in_specs=(
            P("sp", "tp"),
            P(),
            P("sp", "tp"),
            P("sp", "tp"),
            P("sp", "tp"),
            P("sp", "tp"),
            P("sp", "tp"),
            P("sp", "tp"),
            P("sp", "tp"),
            P(None, "tp"),
            P(None, "tp", "sp"),
            P("tp"),
            P("tp", "sp"),
            P("tp", "sp"),
        ),
        out_specs=P(("sp", "tp"), None),
        check_vma=False,
    )
```

```python
import jax
import functools
import jax.numpy as jnp
from jax import lax
from jax.experimental import pallas as pl
from jax.experimental.pallas import tpu as pltpu
from jax.sharding import PartitionSpec as P

HEAD_DIM = 64


EPS = 1e-06
THETA = 10000.0


def with_halo(shard, sides, width):
    for axis, dim in sides:
        size, length = (lax.axis_size(axis), shard.shape[dim])
        up = [(i, (i + 1) % size) for i in range(size - 1)]
        down = [(j, i) for i, j in up]
        last = lax.slice_in_dim(shard, length - width, length, axis=dim)
        first = lax.slice_in_dim(shard, 0, width, axis=dim)
        before = lax.ppermute(last, axis, up)
        after = lax.ppermute(first, axis, down)
        shard = jnp.concatenate([before, shard, after], axis=dim)
    return shard


def rotate(field_in, position_list):
    half_dim = field_in.shape[-1] // 2
    frequency = jnp.exp(
        -jnp.log(THETA) * jnp.arange(half_dim, dtype=jnp.float32) * (2.0 / field_in.shape[-1])
    )
    angles = position_list.astype(jnp.float32)[:, None, None] * frequency
    cosine = jnp.cos(angles)
    sine_part = jnp.sin(angles)
    leading = field_in[..., :half_dim]
    trailing = field_in[..., half_dim:]
    return jnp.concatenate(
        [leading * cosine - trailing * sine_part, leading * sine_part + trailing * cosine], axis=-1
    )


def conv_branch(outer_rows, inner_rows, conv_values, conv_taps):
    inner_value = (inner_rows.astype(jnp.float32) * conv_values.astype(jnp.float32)).astype(
        jnp.bfloat16
    )
    padded = with_halo(inner_value, (("sp", 0),), 1).astype(jnp.float32)
    convolved = conv_taps[0] * padded[:-2] + conv_taps[1] * padded[1:-1] + conv_taps[2] * padded[2:]
    return (outer_rows.astype(jnp.float32) * convolved).astype(jnp.bfloat16)


def span_parts(query_rows, key_rows, value_rows, log_rates):
    length = query_rows.shape[0]
    forward_cum = jnp.cumsum(log_rates[0], axis=-1)
    backward_cum = jnp.flip(jnp.cumsum(jnp.flip(log_rates[1], -1), axis=-1), -1)
    row_index = lax.broadcasted_iota(jnp.int32, (length, length), 0)
    col_index = lax.broadcasted_iota(jnp.int32, (length, length), 1)
    lower_part = (col_index <= row_index)[None]
    spread = jnp.where(
        lower_part,
        forward_cum[:, :, None] - forward_cum[:, None, :],
        backward_cum[:, :, None] - backward_cum[:, None, :],
    )
    scores = jnp.einsum("ihe,jhe->hij", query_rows, key_rows, preferred_element_type=jnp.float32)
    weighted = (scores * jnp.exp(spread)).astype(jnp.bfloat16)
    local_part = jnp.einsum(
        "hij,jhe->ihe", weighted, value_rows, preferred_element_type=jnp.float32
    )
    key_wide = key_rows.astype(jnp.float32)
    forward_keys = (key_wide * jnp.exp(forward_cum[:, -1:] - forward_cum).T[:, :, None]).astype(
        jnp.bfloat16
    )
    backward_keys = (key_wide * jnp.exp(backward_cum[:, :1] - backward_cum).T[:, :, None]).astype(
        jnp.bfloat16
    )
    forward_state = jnp.einsum(
        "jhd,jhe->hde", forward_keys, value_rows, preferred_element_type=jnp.float32
    )
    backward_state = jnp.einsum(
        "jhd,jhe->hde", backward_keys, value_rows, preferred_element_type=jnp.float32
    )
    return (local_part, forward_cum, backward_cum, forward_state, backward_state)


def retention_branch(query_rows, key_rows, value_rows, gate_rows, log_decay, head_gain, offsets):
    row_count = query_rows.shape[0]
    head_count = query_rows.shape[1] // HEAD_DIM
    shape_heads = (row_count, head_count, HEAD_DIM)
    rotated_query = rotate(query_rows.astype(jnp.float32).reshape(shape_heads), offsets).astype(
        jnp.bfloat16
    )
    rotated_key = (
        rotate(key_rows.astype(jnp.float32).reshape(shape_heads), offsets) * HEAD_DIM ** (-0.5)
    ).astype(jnp.bfloat16)
    local_part, forward_cum, backward_cum, forward_state, backward_state = span_parts(
        rotated_query, rotated_key, value_rows.reshape(shape_heads), log_decay
    )
    forward_total = forward_cum[:, -1]
    backward_total = backward_cum[:, 0]
    totals = lax.all_gather(
        jnp.stack([forward_total, backward_total])[None], "sp", axis=0, tiled=True
    )
    inclusive = jnp.cumsum(totals, axis=0)
    exclusive = inclusive - totals
    own_index = lax.axis_index("sp")
    own_inclusive = lax.dynamic_index_in_dim(inclusive, own_index, 0, keepdims=False)
    own_exclusive = lax.dynamic_index_in_dim(exclusive, own_index, 0, keepdims=False)
    pieces = (
        lax.all_gather(forward_state[None], "sp", axis=0, tiled=True),
        lax.all_gather(backward_state[None], "sp", axis=0, tiled=True),
    )
    piece_count = pieces[0].shape[0]
    span_index = lax.iota(jnp.int32, piece_count)
    forward_weight = jnp.where(
        (span_index < own_index)[:, None],
        jnp.exp(jnp.minimum(own_exclusive[0] - inclusive[:, 0], 0.0)),
        0.0,
    )
    backward_weight = jnp.where(
        (span_index > own_index)[:, None],
        jnp.exp(jnp.minimum(exclusive[:, 1] - own_inclusive[1], 0.0)),
        0.0,
    )
    into_forward = jnp.einsum(
        "nh,nhde->hde", forward_weight, pieces[0], precision=lax.Precision.HIGHEST
    )
    into_backward = jnp.einsum(
        "nh,nhde->hde", backward_weight, pieces[1], precision=lax.Precision.HIGHEST
    )
    forward_part = jnp.einsum(
        "ihd,hde->ihe",
        rotated_query,
        into_forward.astype(jnp.bfloat16),
        preferred_element_type=jnp.float32,
    )
    backward_part = jnp.einsum(
        "ihd,hde->ihe",
        rotated_query,
        into_backward.astype(jnp.bfloat16),
        preferred_element_type=jnp.float32,
    )
    mixed_heads = (
        local_part
        + jnp.exp(forward_cum).T[:, :, None] * forward_part
        + jnp.exp(backward_cum).T[:, :, None] * backward_part
    )
    scaled = mixed_heads * lax.rsqrt(
        jnp.mean(mixed_heads * mixed_heads, axis=-1, keepdims=True) + EPS
    )
    scaled = scaled * head_gain.reshape(head_count, HEAD_DIM)
    return (
        jax.nn.silu(gate_rows.astype(jnp.float32))
        * scaled.reshape(row_count, head_count * HEAD_DIM)
    ).astype(jnp.bfloat16)


def local(
    tokens,
    norm_gain,
    outer_gate,
    inner_gate,
    conv_input,
    query_proj,
    key_proj,
    value_proj,
    out_gate,
    conv_taps,
    log_decay,
    head_gain,
    conv_output,
    retention_output,
):
    whole = lax.all_gather(tokens, "tp", axis=1, tiled=True)
    wide = whole.astype(jnp.float32)
    normed = (
        wide * lax.rsqrt(jnp.mean(wide * wide, axis=-1, keepdims=True) + EPS) * norm_gain
    ).astype(jnp.bfloat16)
    row_count = normed.shape[0]
    offsets = lax.axis_index("sp") * row_count + lax.iota(jnp.int32, row_count)
    gathered = (
        lax.all_gather(outer_gate, "sp", axis=0, tiled=True),
        lax.all_gather(inner_gate, "sp", axis=0, tiled=True),
        lax.all_gather(conv_input, "sp", axis=0, tiled=True),
        lax.all_gather(query_proj, "sp", axis=0, tiled=True),
        lax.all_gather(key_proj, "sp", axis=0, tiled=True),
        lax.all_gather(value_proj, "sp", axis=0, tiled=True),
        lax.all_gather(out_gate, "sp", axis=0, tiled=True),
        lax.all_gather(conv_output, "sp", axis=1, tiled=True),
        lax.all_gather(retention_output, "sp", axis=1, tiled=True),
    )
    projected = [
        jnp.dot(normed, weight, preferred_element_type=jnp.float32).astype(jnp.bfloat16)
        for weight in gathered[:7]
    ]
    conv_out = conv_branch(projected[0], projected[1], projected[2], conv_taps)
    ret_out = retention_branch(
        projected[3], projected[4], projected[5], projected[6], log_decay, head_gain, offsets
    )
    conv_weight = gathered[7]
    ret_weight = gathered[8]
    return lax.psum_scatter(
        (
            jnp.dot(conv_out, conv_weight, preferred_element_type=jnp.float32)
            + jnp.dot(ret_out, ret_weight, preferred_element_type=jnp.float32)
        ).astype(jnp.bfloat16),
        "tp",
        scatter_dimension=0,
        tiled=True,
    )


def flipped(place, d):
    if d == 0:
        return place
    if d == 1:
        return place + 1 - 2 * lax.rem(place, 2)
    if d == 2:
        return place + 2 - 4 * lax.rem(lax.div(place, 2), 2)
    return 3 - place


def gather_kernel(
    planes, group, rows_ref, win_ref, wout_ref, rate_ref,
    x_ref, wi_ref, wo_ref, r_ref,
    near_send, near_recv, far_send, far_recv, tok_send, tok_recv, half_send, half_recv, own_sem,
):
    own, core = lax.axis_index("sp"), lax.axis_index("tp")
    place, plane = lax.rem(own, group), lax.div(own, group)
    base = plane * group
    half = rows_ref.shape[1]
    quarter = half // 2
    has_up, has_down = plane < planes - 1, plane > 0
    chips = [base + flipped(place, d) for d in range(group)]

    barrier = pltpu.get_barrier_semaphore()

    def greet(target):
        pl.semaphore_signal(
            barrier, inc=1, device_id=target, device_id_type=pl.DeviceIdType.MESH
        )

    for d in range(1, group):
        greet((chips[d], core))
    greet((own, 1 - core))
    pl.when(has_up)(lambda: greet((own + group, core)))
    pl.when(has_down)(lambda: greet((own - group, core)))
    pl.semaphore_wait(barrier, group + jnp.where(has_up, 1, 0) + jnp.where(has_down, 1, 0))

    def remote(source, target, send, recv, device):
        return pltpu.make_async_remote_copy(
            src_ref=source, dst_ref=target, send_sem=send, recv_sem=recv,
            device_id=device, device_id_type=pl.DeviceIdType.MESH,
        )

    def part(d, which):
        return x_ref.at[d, :, pl.ds(pl.multiple_of(core * half + which * quarter, 128), quarter)]

    def side(d):
        return x_ref.at[d, :, pl.ds(pl.multiple_of(core * half, 128), half)]

    kept = [
        pltpu.make_async_copy(win_ref.at[place], wi_ref.at[plane, place], own_sem.at[0]),
        pltpu.make_async_copy(wout_ref.at[place], wo_ref.at[plane, place], own_sem.at[1]),
        pltpu.make_async_copy(rate_ref.at[place], r_ref.at[0], own_sem.at[2]),
        pltpu.make_async_copy(rows_ref, side(0), own_sem.at[3]),
    ]
    for copy in kept:
        copy.start()

    near = []
    for kind, (source, target) in enumerate(((win_ref, wi_ref), (wout_ref, wo_ref), (rate_ref, r_ref))):
        for d in range(1, group):
            to = flipped(place, d)
            landing = target.at[d] if kind == 2 else target.at[plane, place]
            near.append(
                remote(source.at[to], landing, near_send.at[kind, d], near_recv.at[kind, d], (chips[d], core))
            )
    for copy in near[: group - 1]:
        copy.start()

    def pieces(which):
        return rows_ref.at[:, pl.ds(which * quarter, quarter)]

    tokens = {}

    def send_part(which, source, d_there, hop):
        tokens[(which, d_there)] = remote(
            source, part(d_there, which), tok_send.at[which, d_there], tok_recv.at[which, d_there],
            (chips[hop], core),
        )
        tokens[(which, d_there)].start()

    send_part(0, pieces(0), 1, 1)
    send_part(1, pieces(1), 2, 2)
    send_part(1, pieces(1), 1, 1)
    send_part(0, pieces(0), 2, 2)
    for copy in near[group - 1 :]:
        copy.start()
    partner = (own, 1 - core)
    halves = [remote(rows_ref, side(0), half_send.at[0], half_recv.at[0], partner)]
    halves[0].start()

    def far(kind, ref, direction, k, d):
        q = plane - k if direction == 0 else plane + k
        block = ref.at[q, flipped(place, d)]
        index = (kind, direction, k, d)
        target = own + group if direction == 0 else own - group
        return remote(block, block, far_send.at[index], far_recv.at[index], (target, core))

    def holds(direction, k):
        return plane - k >= 0 if direction == 0 else plane + k < planes

    def forwards(direction, k):
        return jnp.logical_and(holds(direction, k), has_up if direction == 0 else has_down)

    def landed(kind, ref, direction, k, d):
        q = plane - k if direction == 0 else plane + k
        block = ref.at[q, flipped(place, d)]
        index = (kind, direction, k - 1, d)
        remote(block, block, far_send.at[index], far_recv.at[index], (own, 1 - core)).wait_recv()

    def pass_on(kind, ref, k):
        for d in range(group):
            if k == 0:
                if d == 0:
                    kept[kind].wait()
                else:
                    near[kind * (group - 1) + d - 1].wait_recv()
            for direction in range(2):
                if k > 0:
                    pl.when(holds(direction, k))(
                        functools.partial(landed, kind, ref, direction, k, d)
                    )
                if k < planes - 1:
                    pl.when(forwards(direction, k))(
                        lambda direction=direction, d=d: far(kind, ref, direction, k, d).start()
                    )

    pass_on(0, wi_ref, 0)

    tokens[(0, 1)].wait_recv()
    send_part(0, part(1, 0), 3, 2)
    tokens[(1, 2)].wait_recv()
    send_part(1, part(2, 1), 3, 1)
    pass_on(1, wo_ref, 0)
    for which, d in ((1, 1), (0, 2), (0, 3), (1, 3)):
        tokens[(which, d)].wait_recv()
        if (which, d) in ((1, 1), (0, 2)):
            at = d
        elif which == 1:
            at = 3
        else:
            continue
        copy = remote(side(at), side(at), half_send.at[at], half_recv.at[at], partner)
        copy.start()
        halves.append(copy)

    for k in range(1, planes):
        pass_on(0, wi_ref, k)
        pass_on(1, wo_ref, k)

    for copy in kept[2:]:
        copy.wait()
    for copy in near:
        copy.wait_send()
    for copy in near[2 * (group - 1) :]:
        copy.wait_recv()
    for copy in tokens.values():
        copy.wait_send()
    for copy in halves:
        copy.wait()
    for kind, ref in enumerate((wi_ref, wo_ref)):
        for k in range(planes - 1):
            for d in range(group):
                for direction in range(2):
                    pl.when(forwards(direction, k))(
                        lambda kind=kind, ref=ref, direction=direction, k=k, d=d: far(
                            kind, ref, direction, k, d
                        ).wait_send()
                    )


def gather_all(planes, group, rows, weights_in, weights_out, rates):
    length, half = rows.shape
    dma = pltpu.SemaphoreType.DMA
    return pl.pallas_call(
        functools.partial(gather_kernel, planes, group),
        out_shape=(
            jax.ShapeDtypeStruct((group, length, 2 * half), rows.dtype),
            jax.ShapeDtypeStruct((planes,) + weights_in.shape, weights_in.dtype),
            jax.ShapeDtypeStruct((planes,) + weights_out.shape, weights_out.dtype),
            jax.ShapeDtypeStruct(rates.shape, rates.dtype),
        ),
        in_specs=[pl.BlockSpec(memory_space=pl.ANY)] * 4,
        out_specs=[pl.BlockSpec(memory_space=pl.ANY)] * 4,
        scratch_shapes=[
            dma((3, group)), dma((3, group)),
            dma((2, 2, planes, group)), dma((2, 2, planes, group)),
            dma((2, group)), dma((2, group)),
            dma((group,)), dma((group,)),
            dma((4,)),
        ],
        compiler_params=pltpu.CompilerParams(collective_id=0, has_side_effects=True),
    )(rows, weights_in, weights_out, rates)


def plane_local(planes, group, arrays):
    (
        tokens,
        norm_gain,
        outer_gate,
        inner_gate,
        conv_input,
        query_proj,
        key_proj,
        value_proj,
        out_gate,
        conv_taps,
        log_decay,
        head_gain,
        conv_output,
        retention_output,
    ) = arrays
    spans = planes * group
    own = lax.axis_index("sp")
    core = lax.axis_index("tp")
    place = lax.rem(own, group)
    plane = lax.div(own, group)
    length, half_width = tokens.shape
    width = half_width * 2
    channels = outer_gate.shape[1] // group
    heads = channels // HEAD_DIM
    f32, bf16 = jnp.float32, jnp.bfloat16

    def swap(x, d):
        return lax.ppermute(x, "sp", [(i, i ^ d) for i in range(spans)])

    def up(x, k=1):
        return lax.ppermute(x, "sp", [(i, i + k * group) for i in range(spans - k * group)])

    def down(x, k=1):
        return lax.ppermute(x, "sp", [(i + k * group, i) for i in range(spans - k * group)])

    def cross(x):
        return lax.ppermute(x, "tp", [(0, 1), (1, 0)])

    def pick(x, index, axis=0):
        return lax.dynamic_index_in_dim(x, index, axis, keepdims=False)

    def reorder(pieces):
        stacked = jnp.stack(pieces) if isinstance(pieces, (list, tuple)) else pieces
        return jnp.stack([pick(stacked, jnp.bitwise_xor(place, t)) for t in range(group)])

    wide = tokens.astype(f32)
    square_sum = jnp.sum(wide * wide, axis=-1).reshape(-1, 128)
    square_sum = (square_sum + cross(square_sum)).reshape(length, 1)
    own_gain = lax.dynamic_slice_in_dim(norm_gain, core * half_width, half_width)
    normed = (wide * lax.rsqrt(square_sum / width + EPS) * own_gain).astype(bf16)

    rows_in = outer_gate.shape[0]
    weights_in = jnp.stack(
        [
            w.reshape(rows_in, group, channels)
            for w in (key_proj, query_proj, value_proj, inner_gate, conv_input, outer_gate, out_gate)
        ],
        axis=2,
    ).reshape(rows_in, group, 7 * channels).transpose(1, 0, 2)
    out_cols = conv_output.shape[1]
    weights_out = jnp.concatenate(
        [w.reshape(group, channels, out_cols) for w in (conv_output, retention_output)], axis=1
    )
    own_rates = log_decay.reshape(2, group, heads, length).transpose(1, 0, 2, 3)
    rows_all, win_all, wout_all, rates = gather_all(
        planes, group, normed, weights_in, weights_out, own_rates.reshape(group, 2 * heads, length)
    )
    rates = rates.reshape(group, 2, heads, length)
    projected = jnp.dot(
        rows_all.reshape(group * length, width),
        win_all.reshape(width, 7 * channels),
        preferred_element_type=f32,
    ).astype(bf16)
    out_weight = wout_all.transpose(2, 0, 1, 3).reshape(2 * channels, width)

    span_ids = plane * group + jnp.bitwise_xor(place, lax.iota(jnp.int32, group))
    positions = (span_ids[:, None] * length + lax.iota(jnp.int32, length)).reshape(-1)
    half_dim = HEAD_DIM // 2
    frequency = jnp.exp(
        -jnp.log(THETA) * jnp.arange(half_dim, dtype=f32) * (2.0 / HEAD_DIM)
    )
    angles = positions.astype(f32)[:, None] * frequency
    cosine, sine = lax.optimization_barrier((jnp.cos(angles), jnp.sin(angles)))
    cosine, sine = cosine[:, None, :], sine[:, None, :]

    def turned(x):
        x = x.astype(f32).reshape(group * length, heads, HEAD_DIM)
        a, b = x[..., :half_dim], x[..., half_dim:]
        return jnp.concatenate([a * cosine - b * sine, a * sine + b * cosine], axis=-1)

    shape_heads = (group, length, heads, HEAD_DIM)
    kqv, rest = projected[:, : 3 * channels], projected[:, 3 * channels :]
    rk = (turned(kqv[:, :channels]) * HEAD_DIM ** (-0.5)).astype(bf16).reshape(shape_heads)
    rq = turned(kqv[:, channels : 2 * channels]).astype(bf16).reshape(shape_heads)
    value = kqv[:, 2 * channels :].reshape(shape_heads)
    local_part, forward_cum, backward_cum, forward_state, backward_state = jax.vmap(span_parts)(
        rq, rk, value, rates
    )
    forward_total = reorder(forward_cum[:, :, -1])
    backward_total = reorder(backward_cum[:, :, 0])
    forward_state = reorder(forward_state)
    backward_state = reorder(backward_state)

    def carry(states, totals, send):
        running = jnp.zeros_like(states[0])
        passed = jnp.zeros_like(totals[0])
        inside, reach = [], []
        for t in range(group):
            inside.append(running)
            reach.append(passed)
            running = jnp.exp(totals[t])[:, None, None] * running + states[t]
            passed = passed + totals[t]
        incoming, between = jnp.zeros_like(running), jnp.zeros_like(passed)
        for k in range(1, planes):
            incoming = incoming + jnp.exp(between)[:, None, None] * send(running, k)
            if k + 1 < planes:
                between = between + send(passed, k)
        return [
            a + jnp.exp(b)[:, None, None] * incoming for a, b in zip(inside, reach)
        ]

    into_forward = carry(list(forward_state), list(forward_total), up)
    into_backward = carry(list(backward_state)[::-1], list(backward_total)[::-1], down)[::-1]
    into_forward = reorder(into_forward).astype(bf16)
    into_backward = reorder(into_backward).astype(bf16)

    inner_value = (
        rest[:, :channels].astype(f32) * rest[:, channels : 2 * channels].astype(f32)
    ).astype(bf16).reshape(group, length, channels)
    lasts = reorder(inner_value[:, -1:])
    firsts = reorder(inner_value[:, :1])
    before = reorder(jnp.concatenate([up(lasts[-1:]), lasts[:-1]], axis=0))
    after = reorder(jnp.concatenate([firsts[1:], down(firsts[:1])], axis=0))
    taps = lax.dynamic_slice_in_dim(conv_taps, place * channels, channels, axis=1)
    padded = jnp.concatenate([before, inner_value, after], axis=1).astype(f32)
    convolved = taps[0] * padded[:, :-2] + taps[1] * padded[:, 1:-1] + taps[2] * padded[:, 2:]
    outer = rest[:, 2 * channels : 3 * channels].reshape(group, length, channels)
    conv_out = (outer.astype(f32) * convolved).astype(bf16)

    forward_part = jnp.einsum("sihd,shde->sihe", rq, into_forward, preferred_element_type=f32)
    backward_part = jnp.einsum("sihd,shde->sihe", rq, into_backward, preferred_element_type=f32)
    mixed_heads = (
        local_part
        + jnp.exp(forward_cum).transpose(0, 2, 1)[..., None] * forward_part
        + jnp.exp(backward_cum).transpose(0, 2, 1)[..., None] * backward_part
    )
    scaled = mixed_heads * lax.rsqrt(
        jnp.mean(mixed_heads * mixed_heads, axis=-1, keepdims=True) + EPS
    )
    own_head_gain = lax.dynamic_slice_in_dim(head_gain, place * channels, channels)
    scaled = scaled.reshape(group, length, channels) * own_head_gain
    gate = rest[:, 3 * channels :].reshape(group, length, channels)
    ret_out = (jax.nn.silu(gate.astype(f32)) * scaled).astype(bf16)

    features = jnp.concatenate([conv_out, ret_out], axis=-1)
    features = features.reshape(group, 2, length // 2, 2 * channels)
    mine_rows, their_rows = pick(features, core, 1), pick(features, 1 - core, 1)
    half_out = out_weight.shape[1] // 2

    def partial(rows, ids, weight):
        picked = jnp.concatenate([rows[i] for i in ids], axis=0)
        return jnp.dot(picked, weight, preferred_element_type=f32)

    def chip_sum(ids, weight):
        theirs = cross(partial(their_rows, ids, weight).astype(bf16))
        total = partial(mine_rows, ids, weight) + theirs.astype(f32)
        return total.reshape(len(ids), length // 2, half_out)

    def scatter(weight, one, two):
        sent = swap(chip_sum((one, one ^ two), weight).astype(bf16), one)
        kept = chip_sum((0, two), weight) + sent.astype(f32)
        return kept[0] + swap(kept[1].astype(bf16), two).astype(f32)

    return jnp.concatenate(
        [
            scatter(out_weight[:, :half_out], 1, 2),
            scatter(out_weight[:, half_out:], 2, 1),
        ],
        axis=1,
    ).astype(bf16)


LANES = 128


def plan(*arrays):
    spans, cores = lax.axis_size("sp"), lax.axis_size("tp")
    group = arrays[2].shape[1] // LANES
    planes = spans // group
    fits = (
        cores == 2
        and group == 4
        and planes * group == spans
        and planes == 2 * cores
        and arrays[0].shape[1] == 2 * group * arrays[2].shape[0]
    )
    return plane_local(planes, group, arrays) if fits else local(*arrays)


def solution(mesh):
    return jax.shard_map(
        plan,
        mesh=mesh,
        in_specs=(
            P("sp", "tp"),
            P(),
            P("sp", "tp"),
            P("sp", "tp"),
            P("sp", "tp"),
            P("sp", "tp"),
            P("sp", "tp"),
            P("sp", "tp"),
            P("sp", "tp"),
            P(None, "tp"),
            P(None, "tp", "sp"),
            P("tp"),
            P("tp", "sp"),
            P("tp", "sp"),
        ),
        out_specs=P(("sp", "tp"), None),
        check_vma=False,
    )
```

```python
import jax
import functools
import jax.numpy as jnp
from jax import lax
from jax.experimental import pallas as pl
from jax.experimental.pallas import tpu as pltpu
from jax.sharding import PartitionSpec as P

HEAD_DIM = 64


EPS = 1e-06
THETA = 10000.0


def with_halo(shard, sides, width):
    for axis, dim in sides:
        size, length = (lax.axis_size(axis), shard.shape[dim])
        up = [(i, (i + 1) % size) for i in range(size - 1)]
        down = [(j, i) for i, j in up]
        last = lax.slice_in_dim(shard, length - width, length, axis=dim)
        first = lax.slice_in_dim(shard, 0, width, axis=dim)
        before = lax.ppermute(last, axis, up)
        after = lax.ppermute(first, axis, down)
        shard = jnp.concatenate([before, shard, after], axis=dim)
    return shard


def rotate(field_in, position_list):
    half_dim = field_in.shape[-1] // 2
    frequency = jnp.exp(
        -jnp.log(THETA) * jnp.arange(half_dim, dtype=jnp.float32) * (2.0 / field_in.shape[-1])
    )
    angles = position_list.astype(jnp.float32)[:, None, None] * frequency
    cosine = jnp.cos(angles)
    sine_part = jnp.sin(angles)
    leading = field_in[..., :half_dim]
    trailing = field_in[..., half_dim:]
    return jnp.concatenate(
        [leading * cosine - trailing * sine_part, leading * sine_part + trailing * cosine], axis=-1
    )


def conv_branch(outer_rows, inner_rows, conv_values, conv_taps):
    inner_value = (inner_rows.astype(jnp.float32) * conv_values.astype(jnp.float32)).astype(
        jnp.bfloat16
    )
    padded = with_halo(inner_value, (("sp", 0),), 1).astype(jnp.float32)
    convolved = conv_taps[0] * padded[:-2] + conv_taps[1] * padded[1:-1] + conv_taps[2] * padded[2:]
    return (outer_rows.astype(jnp.float32) * convolved).astype(jnp.bfloat16)


def span_parts(query_rows, key_rows, value_rows, log_rates):
    length = query_rows.shape[0]
    forward_cum = jnp.cumsum(log_rates[0], axis=-1)
    backward_cum = jnp.flip(jnp.cumsum(jnp.flip(log_rates[1], -1), axis=-1), -1)
    row_index = lax.broadcasted_iota(jnp.int32, (length, length), 0)
    col_index = lax.broadcasted_iota(jnp.int32, (length, length), 1)
    lower_part = (col_index <= row_index)[None]
    spread = jnp.where(
        lower_part,
        forward_cum[:, :, None] - forward_cum[:, None, :],
        backward_cum[:, :, None] - backward_cum[:, None, :],
    )
    scores = jnp.einsum("ihe,jhe->hij", query_rows, key_rows, preferred_element_type=jnp.float32)
    weighted = (scores * jnp.exp(spread)).astype(jnp.bfloat16)
    local_part = jnp.einsum(
        "hij,jhe->ihe", weighted, value_rows, preferred_element_type=jnp.float32
    )
    key_wide = key_rows.astype(jnp.float32)
    forward_keys = (key_wide * jnp.exp(forward_cum[:, -1:] - forward_cum).T[:, :, None]).astype(
        jnp.bfloat16
    )
    backward_keys = (key_wide * jnp.exp(backward_cum[:, :1] - backward_cum).T[:, :, None]).astype(
        jnp.bfloat16
    )
    forward_state = jnp.einsum(
        "jhd,jhe->hde", forward_keys, value_rows, preferred_element_type=jnp.float32
    )
    backward_state = jnp.einsum(
        "jhd,jhe->hde", backward_keys, value_rows, preferred_element_type=jnp.float32
    )
    return (local_part, forward_cum, backward_cum, forward_state, backward_state)


def retention_branch(query_rows, key_rows, value_rows, gate_rows, log_decay, head_gain, offsets):
    row_count = query_rows.shape[0]
    head_count = query_rows.shape[1] // HEAD_DIM
    shape_heads = (row_count, head_count, HEAD_DIM)
    rotated_query = rotate(query_rows.astype(jnp.float32).reshape(shape_heads), offsets).astype(
        jnp.bfloat16
    )
    rotated_key = (
        rotate(key_rows.astype(jnp.float32).reshape(shape_heads), offsets) * HEAD_DIM ** (-0.5)
    ).astype(jnp.bfloat16)
    local_part, forward_cum, backward_cum, forward_state, backward_state = span_parts(
        rotated_query, rotated_key, value_rows.reshape(shape_heads), log_decay
    )
    forward_total = forward_cum[:, -1]
    backward_total = backward_cum[:, 0]
    totals = lax.all_gather(
        jnp.stack([forward_total, backward_total])[None], "sp", axis=0, tiled=True
    )
    inclusive = jnp.cumsum(totals, axis=0)
    exclusive = inclusive - totals
    own_index = lax.axis_index("sp")
    own_inclusive = lax.dynamic_index_in_dim(inclusive, own_index, 0, keepdims=False)
    own_exclusive = lax.dynamic_index_in_dim(exclusive, own_index, 0, keepdims=False)
    pieces = (
        lax.all_gather(forward_state[None], "sp", axis=0, tiled=True),
        lax.all_gather(backward_state[None], "sp", axis=0, tiled=True),
    )
    piece_count = pieces[0].shape[0]
    span_index = lax.iota(jnp.int32, piece_count)
    forward_weight = jnp.where(
        (span_index < own_index)[:, None],
        jnp.exp(jnp.minimum(own_exclusive[0] - inclusive[:, 0], 0.0)),
        0.0,
    )
    backward_weight = jnp.where(
        (span_index > own_index)[:, None],
        jnp.exp(jnp.minimum(exclusive[:, 1] - own_inclusive[1], 0.0)),
        0.0,
    )
    into_forward = jnp.einsum(
        "nh,nhde->hde", forward_weight, pieces[0], precision=lax.Precision.HIGHEST
    )
    into_backward = jnp.einsum(
        "nh,nhde->hde", backward_weight, pieces[1], precision=lax.Precision.HIGHEST
    )
    forward_part = jnp.einsum(
        "ihd,hde->ihe",
        rotated_query,
        into_forward.astype(jnp.bfloat16),
        preferred_element_type=jnp.float32,
    )
    backward_part = jnp.einsum(
        "ihd,hde->ihe",
        rotated_query,
        into_backward.astype(jnp.bfloat16),
        preferred_element_type=jnp.float32,
    )
    mixed_heads = (
        local_part
        + jnp.exp(forward_cum).T[:, :, None] * forward_part
        + jnp.exp(backward_cum).T[:, :, None] * backward_part
    )
    scaled = mixed_heads * lax.rsqrt(
        jnp.mean(mixed_heads * mixed_heads, axis=-1, keepdims=True) + EPS
    )
    scaled = scaled * head_gain.reshape(head_count, HEAD_DIM)
    return (
        jax.nn.silu(gate_rows.astype(jnp.float32))
        * scaled.reshape(row_count, head_count * HEAD_DIM)
    ).astype(jnp.bfloat16)


def local(
    tokens,
    norm_gain,
    outer_gate,
    inner_gate,
    conv_input,
    query_proj,
    key_proj,
    value_proj,
    out_gate,
    conv_taps,
    log_decay,
    head_gain,
    conv_output,
    retention_output,
):
    whole = lax.all_gather(tokens, "tp", axis=1, tiled=True)
    wide = whole.astype(jnp.float32)
    normed = (
        wide * lax.rsqrt(jnp.mean(wide * wide, axis=-1, keepdims=True) + EPS) * norm_gain
    ).astype(jnp.bfloat16)
    row_count = normed.shape[0]
    offsets = lax.axis_index("sp") * row_count + lax.iota(jnp.int32, row_count)
    gathered = (
        lax.all_gather(outer_gate, "sp", axis=0, tiled=True),
        lax.all_gather(inner_gate, "sp", axis=0, tiled=True),
        lax.all_gather(conv_input, "sp", axis=0, tiled=True),
        lax.all_gather(query_proj, "sp", axis=0, tiled=True),
        lax.all_gather(key_proj, "sp", axis=0, tiled=True),
        lax.all_gather(value_proj, "sp", axis=0, tiled=True),
        lax.all_gather(out_gate, "sp", axis=0, tiled=True),
        lax.all_gather(conv_output, "sp", axis=1, tiled=True),
        lax.all_gather(retention_output, "sp", axis=1, tiled=True),
    )
    projected = [
        jnp.dot(normed, weight, preferred_element_type=jnp.float32).astype(jnp.bfloat16)
        for weight in gathered[:7]
    ]
    conv_out = conv_branch(projected[0], projected[1], projected[2], conv_taps)
    ret_out = retention_branch(
        projected[3], projected[4], projected[5], projected[6], log_decay, head_gain, offsets
    )
    conv_weight = gathered[7]
    ret_weight = gathered[8]
    return lax.psum_scatter(
        (
            jnp.dot(conv_out, conv_weight, preferred_element_type=jnp.float32)
            + jnp.dot(ret_out, ret_weight, preferred_element_type=jnp.float32)
        ).astype(jnp.bfloat16),
        "tp",
        scatter_dimension=0,
        tiled=True,
    )


def flipped(place, d):
    if d == 0:
        return place
    if d == 1:
        return place + 1 - 2 * lax.rem(place, 2)
    if d == 2:
        return place + 2 - 4 * lax.rem(lax.div(place, 2), 2)
    return 3 - place


def gather_kernel(
    planes, group, rows_ref, win_ref, later_ref, rate_ref,
    x_ref, wi_ref, lo_ref, r_ref,
    near_send, near_recv, far_send, far_recv, tok_send, tok_recv, half_send, half_recv, own_sem,
):
    own, core = lax.axis_index("sp"), lax.axis_index("tp")
    place, plane = lax.rem(own, group), lax.div(own, group)
    base = plane * group
    half = rows_ref.shape[1]
    quarter = half // 2
    has_up, has_down = plane < planes - 1, plane > 0
    chips = [base + flipped(place, d) for d in range(group)]

    barrier = pltpu.get_barrier_semaphore()

    def greet(target):
        pl.semaphore_signal(
            barrier, inc=1, device_id=target, device_id_type=pl.DeviceIdType.MESH
        )

    for d in range(1, group):
        greet((chips[d], core))
    greet((own, 1 - core))
    pl.when(has_up)(lambda: greet((own + group, core)))
    pl.when(has_down)(lambda: greet((own - group, core)))
    pl.semaphore_wait(barrier, group + jnp.where(has_up, 1, 0) + jnp.where(has_down, 1, 0))

    def remote(source, target, send, recv, device):
        return pltpu.make_async_remote_copy(
            src_ref=source, dst_ref=target, send_sem=send, recv_sem=recv,
            device_id=device, device_id_type=pl.DeviceIdType.MESH,
        )

    def part(d, which):
        return x_ref.at[d, :, pl.ds(pl.multiple_of(core * half + which * quarter, 128), quarter)]

    def side(d):
        return x_ref.at[d, :, pl.ds(pl.multiple_of(core * half, 128), half)]

    kept = [
        pltpu.make_async_copy(win_ref.at[place], wi_ref.at[plane, place], own_sem.at[0]),
        pltpu.make_async_copy(later_ref.at[place], lo_ref.at[place], own_sem.at[1]),
        pltpu.make_async_copy(rate_ref.at[place], r_ref.at[0], own_sem.at[2]),
        pltpu.make_async_copy(rows_ref, side(0), own_sem.at[3]),
    ]
    for copy in kept:
        copy.start()

    near = []
    for kind, (source, target) in enumerate(((win_ref, wi_ref), (later_ref, lo_ref), (rate_ref, r_ref))):
        for d in range(1, group):
            to = flipped(place, d)
            landing = (target.at[plane, place], target.at[place], target.at[d])[kind]
            near.append(
                remote(source.at[to], landing, near_send.at[kind, d], near_recv.at[kind, d], (chips[d], core))
            )
    for copy in near[: group - 1]:
        copy.start()

    def pieces(which):
        return rows_ref.at[:, pl.ds(which * quarter, quarter)]

    tokens = {}

    def send_part(which, source, d_there, hop):
        tokens[(which, d_there)] = remote(
            source, part(d_there, which), tok_send.at[which, d_there], tok_recv.at[which, d_there],
            (chips[hop], core),
        )
        tokens[(which, d_there)].start()

    send_part(0, pieces(0), 1, 1)
    send_part(1, pieces(1), 2, 2)
    send_part(1, pieces(1), 1, 1)
    send_part(0, pieces(0), 2, 2)
    for copy in near[group - 1 :]:
        copy.start()
    partner = (own, 1 - core)
    halves = [remote(rows_ref, side(0), half_send.at[0], half_recv.at[0], partner)]
    halves[0].start()

    def far(kind, ref, direction, k, d):
        q = plane - k if direction == 0 else plane + k
        block = ref.at[q, flipped(place, d)]
        index = (kind, direction, k, d)
        target = own + group if direction == 0 else own - group
        return remote(block, block, far_send.at[index], far_recv.at[index], (target, core))

    def holds(direction, k):
        return plane - k >= 0 if direction == 0 else plane + k < planes

    def forwards(direction, k):
        return jnp.logical_and(holds(direction, k), has_up if direction == 0 else has_down)

    def landed(kind, ref, direction, k, d):
        q = plane - k if direction == 0 else plane + k
        block = ref.at[q, flipped(place, d)]
        index = (kind, direction, k - 1, d)
        remote(block, block, far_send.at[index], far_recv.at[index], (own, 1 - core)).wait_recv()

    def pass_on(kind, ref, k):
        for d in range(group):
            if k == 0:
                if d == 0:
                    kept[kind].wait()
                else:
                    near[kind * (group - 1) + d - 1].wait_recv()
            for direction in range(2):
                if k > 0:
                    pl.when(holds(direction, k))(
                        functools.partial(landed, kind, ref, direction, k, d)
                    )
                if k < planes - 1:
                    pl.when(forwards(direction, k))(
                        lambda direction=direction, d=d: far(kind, ref, direction, k, d).start()
                    )

    pass_on(0, wi_ref, 0)

    tokens[(0, 1)].wait_recv()
    send_part(0, part(1, 0), 3, 2)
    tokens[(1, 2)].wait_recv()
    send_part(1, part(2, 1), 3, 1)
    for which, d in ((1, 1), (0, 2), (0, 3), (1, 3)):
        tokens[(which, d)].wait_recv()
        if (which, d) in ((1, 1), (0, 2)):
            at = d
        elif which == 1:
            at = 3
        else:
            continue
        copy = remote(side(at), side(at), half_send.at[at], half_recv.at[at], partner)
        copy.start()
        halves.append(copy)

    for k in range(1, planes):
        pass_on(0, wi_ref, k)

    for copy in kept[1:]:
        copy.wait()
    for copy in near:
        copy.wait_send()
    for copy in near[group - 1 :]:
        copy.wait_recv()
    for copy in tokens.values():
        copy.wait_send()
    for copy in halves:
        copy.wait()
    for kind, ref in enumerate((wi_ref,)):
        for k in range(planes - 1):
            for d in range(group):
                for direction in range(2):
                    pl.when(forwards(direction, k))(
                        lambda kind=kind, ref=ref, direction=direction, k=k, d=d: far(
                            kind, ref, direction, k, d
                        ).wait_send()
                    )


def gather_all(planes, group, rows, weights_in, later, rates):
    length, half = rows.shape
    dma = pltpu.SemaphoreType.DMA
    return pl.pallas_call(
        functools.partial(gather_kernel, planes, group),
        out_shape=(
            jax.ShapeDtypeStruct((group, length, 2 * half), rows.dtype),
            jax.ShapeDtypeStruct((planes,) + weights_in.shape, weights_in.dtype),
            jax.ShapeDtypeStruct(later.shape, later.dtype),
            jax.ShapeDtypeStruct(rates.shape, rates.dtype),
        ),
        in_specs=[pl.BlockSpec(memory_space=pl.ANY)] * 4,
        out_specs=[pl.BlockSpec(memory_space=pl.ANY)] * 4,
        scratch_shapes=[
            dma((3, group)), dma((3, group)),
            dma((1, 2, planes, group)), dma((1, 2, planes, group)),
            dma((2, group)), dma((2, group)),
            dma((group,)), dma((group,)),
            dma((4,)),
        ],
        compiler_params=pltpu.CompilerParams(collective_id=0, has_side_effects=True),
    )(rows, weights_in, later, rates)


def line_kernel(planes, group, f_ref, b_ref, of_ref, ob_ref, send, recv):
    own, core = lax.axis_index("sp"), lax.axis_index("tp")
    plane = lax.div(own, group)
    barrier = pltpu.get_barrier_semaphore()
    mesh_id = pl.DeviceIdType.MESH

    def greet(target):
        pl.semaphore_signal(barrier, inc=1, device_id=(target, core), device_id_type=mesh_id)

    moves = []
    for k in range(1, planes):
        ahead, behind = plane + k < planes, plane - k >= 0
        pl.when(ahead)(functools.partial(greet, own + k * group))
        pl.when(behind)(functools.partial(greet, own - k * group))
        forward = functools.partial(
            pltpu.make_async_remote_copy,
            src_ref=f_ref, dst_ref=of_ref.at[k - 1], send_sem=send.at[0, k], recv_sem=recv.at[0, k],
            device_id_type=mesh_id,
        )
        backward = functools.partial(
            pltpu.make_async_remote_copy,
            src_ref=b_ref, dst_ref=ob_ref.at[k - 1], send_sem=send.at[1, k], recv_sem=recv.at[1, k],
            device_id_type=mesh_id,
        )
        moves.append((forward, ahead, behind, own + k * group, own - k * group))
        moves.append((backward, behind, ahead, own - k * group, own + k * group))
    pl.semaphore_wait(barrier, planes - 1)
    for make, gives, _, target, _ in moves:
        pl.when(gives)(lambda make=make, target=target: make(device_id=(target, core)).start())
    for make, gives, takes, target, source in moves:
        pl.when(takes)(lambda make=make, source=source: make(device_id=(source, core)).wait_recv())
        pl.when(gives)(lambda make=make, target=target: make(device_id=(target, core)).wait_send())


def pass_line(planes, group, forward, backward):
    out = jax.ShapeDtypeStruct((planes - 1,) + forward.shape, forward.dtype)
    vmem = pl.BlockSpec(memory_space=pltpu.VMEM)
    return pl.pallas_call(
        functools.partial(line_kernel, planes, group),
        out_shape=(out, out),
        in_specs=[vmem] * 2,
        out_specs=[vmem] * 2,
        scratch_shapes=[pltpu.SemaphoreType.DMA((2, planes))] * 2,
        compiler_params=pltpu.CompilerParams(collective_id=1, has_side_effects=True),
    )(forward, backward)


def plane_local(planes, group, arrays):
    (
        tokens,
        norm_gain,
        outer_gate,
        inner_gate,
        conv_input,
        query_proj,
        key_proj,
        value_proj,
        out_gate,
        conv_taps,
        log_decay,
        head_gain,
        conv_output,
        retention_output,
    ) = arrays
    spans = planes * group
    own = lax.axis_index("sp")
    core = lax.axis_index("tp")
    place = lax.rem(own, group)
    plane = lax.div(own, group)
    length, half_width = tokens.shape
    width = half_width * 2
    channels = outer_gate.shape[1] // group
    heads = channels // HEAD_DIM
    f32, bf16 = jnp.float32, jnp.bfloat16

    def swap(x, d):
        return lax.ppermute(x, "sp", [(i, i ^ d) for i in range(spans)])

    def up(x, k=1):
        return lax.ppermute(x, "sp", [(i, i + k * group) for i in range(spans - k * group)])

    def down(x, k=1):
        return lax.ppermute(x, "sp", [(i + k * group, i) for i in range(spans - k * group)])

    def cross(x):
        return lax.ppermute(x, "tp", [(0, 1), (1, 0)])

    def pick(x, index, axis=0):
        return lax.dynamic_index_in_dim(x, index, axis, keepdims=False)

    def reorder(pieces):
        stacked = jnp.stack(pieces) if isinstance(pieces, (list, tuple)) else pieces
        return jnp.stack([pick(stacked, jnp.bitwise_xor(place, t)) for t in range(group)])

    wide = tokens.astype(f32)
    square_sum = jnp.sum(wide * wide, axis=-1).reshape(-1, 128)
    square_sum = (square_sum + cross(square_sum)).reshape(length, 1)
    own_gain = lax.dynamic_slice_in_dim(norm_gain, core * half_width, half_width)
    normed = (wide * lax.rsqrt(square_sum / width + EPS) * own_gain).astype(bf16)

    rows_in = outer_gate.shape[0]

    def by_place(weights):
        stacked = jnp.stack([w.reshape(rows_in, group, channels) for w in weights], axis=2)
        return stacked.reshape(rows_in, group, len(weights) * channels).transpose(1, 0, 2)

    later = jnp.concatenate(
        [
            by_place((inner_gate, conv_input, outer_gate, out_gate)),
            conv_output.reshape(group, channels, -1),
            retention_output.reshape(group, channels, -1),
        ],
        axis=2,
    )
    own_rates = log_decay.reshape(2, group, heads, length).transpose(1, 0, 2, 3)
    rows_all, win_all, later, rates = gather_all(
        planes,
        group,
        normed,
        by_place((key_proj, query_proj, value_proj)),
        later,
        own_rates.reshape(group, 2 * heads, length),
    )
    rates = rates.reshape(group, 2, heads, length)
    rows_all = rows_all.reshape(group * length, width)
    kqv = jnp.dot(
        rows_all, win_all.reshape(width, 3 * channels), preferred_element_type=f32
    ).astype(bf16)

    ups, downs = [later], [later]
    for _ in range(planes - 1):
        ups.append(up(ups[-1]))
        downs.append(down(downs[-1]))
    found = jnp.stack(
        [later]
        + [jnp.where(plane + o < planes, downs[o], ups[planes - o]) for o in range(1, planes)]
    )
    found = jnp.stack(
        [pick(found, lax.rem(t - plane + planes, planes)) for t in range(planes)]
    )
    rest_weight = found[..., : 4 * channels].reshape(width, 4 * channels)
    out_weight = jnp.concatenate(
        [
            found[..., i * channels : (i + 1) * channels]
            .transpose(2, 0, 1, 3)
            .reshape(channels, width)
            for i in (4, 5)
        ],
        axis=0,
    )

    span_ids = plane * group + jnp.bitwise_xor(place, lax.iota(jnp.int32, group))
    positions = (span_ids[:, None] * length + lax.iota(jnp.int32, length)).reshape(-1)
    half_dim = HEAD_DIM // 2
    frequency = jnp.exp(
        -jnp.log(THETA) * jnp.arange(half_dim, dtype=f32) * (2.0 / HEAD_DIM)
    )
    angles = positions.astype(f32)[:, None] * frequency
    cosine, sine = lax.optimization_barrier((jnp.cos(angles), jnp.sin(angles)))
    cosine, sine = cosine[:, None, :], sine[:, None, :]

    def turned(x):
        x = x.astype(f32).reshape(group * length, heads, HEAD_DIM)
        a, b = x[..., :half_dim], x[..., half_dim:]
        return jnp.concatenate([a * cosine - b * sine, a * sine + b * cosine], axis=-1)

    shape_heads = (group, length, heads, HEAD_DIM)
    rk = (turned(kqv[:, :channels]) * HEAD_DIM ** (-0.5)).astype(bf16).reshape(shape_heads)
    rq = turned(kqv[:, channels : 2 * channels]).astype(bf16).reshape(shape_heads)
    value = kqv[:, 2 * channels :].reshape(shape_heads)
    local_part, forward_cum, backward_cum, forward_state, backward_state = jax.vmap(span_parts)(
        rq, rk, value, rates
    )
    forward_total = reorder(forward_cum[:, :, -1])
    backward_total = reorder(backward_cum[:, :, 0])
    forward_state = reorder(forward_state)
    backward_state = reorder(backward_state)

    rest = jnp.dot(rows_all, rest_weight, preferred_element_type=f32).astype(bf16)
    inner_value = (
        rest[:, :channels].astype(f32) * rest[:, channels : 2 * channels].astype(f32)
    ).astype(bf16).reshape(group, length, channels)
    lasts = reorder(inner_value[:, -1:])
    firsts = reorder(inner_value[:, :1])

    def gather_up(states, totals, edge):
        running = jnp.zeros_like(states[0])
        passed = jnp.zeros_like(totals[0])
        inside, reach = [], []
        for state, total in zip(states, totals):
            inside.append(running)
            reach.append(passed)
            running = jnp.exp(total)[:, None, None] * running + state
            passed = passed + total
        body = running.reshape(-1, channels)
        row = jnp.pad(passed, (0, channels - heads))[None]
        rows = [body, row, edge.astype(f32)]
        return inside, reach, jnp.pad(jnp.concatenate(rows, axis=0), ((0, 6), (0, 0)))

    def finish_carry(inside, reach, packs, exists):
        packs = [jnp.where(e, p, 0.0) for e, p in zip(exists, packs)]
        count = heads * HEAD_DIM * HEAD_DIM // channels
        incoming, between = jnp.zeros_like(inside[0]), jnp.zeros_like(reach[0])
        for pack in packs:
            state = pack[:count].reshape(heads, HEAD_DIM, HEAD_DIM)
            incoming = incoming + jnp.exp(between)[:, None, None] * state
            between = between + pack[count, :heads]
        into = [a + jnp.exp(b)[:, None, None] * incoming for a, b in zip(inside, reach)]
        return into, packs[0][count + 1][None, None].astype(bf16)

    forward_in, forward_reach, forward_pack = gather_up(
        list(forward_state), list(forward_total), lasts[-1]
    )
    backward_in, backward_reach, backward_pack = gather_up(
        list(backward_state)[::-1], list(backward_total)[::-1], firsts[0]
    )
    forward_got, backward_got = pass_line(planes, group, forward_pack, backward_pack)
    steps = range(1, planes)
    into_forward, edge_before = finish_carry(
        forward_in, forward_reach, list(forward_got), [plane - k >= 0 for k in steps]
    )
    into_backward, edge_after = finish_carry(
        backward_in, backward_reach, list(backward_got), [plane + k < planes for k in steps]
    )
    into_forward = reorder(into_forward).astype(bf16)
    into_backward = reorder(into_backward[::-1]).astype(bf16)
    before = reorder(jnp.concatenate([edge_before, lasts[:-1]], axis=0))
    after = reorder(jnp.concatenate([firsts[1:], edge_after], axis=0))
    taps = lax.dynamic_slice_in_dim(conv_taps, place * channels, channels, axis=1)
    padded = jnp.concatenate([before, inner_value, after], axis=1).astype(f32)
    convolved = taps[0] * padded[:, :-2] + taps[1] * padded[:, 1:-1] + taps[2] * padded[:, 2:]
    outer = rest[:, 2 * channels : 3 * channels].reshape(group, length, channels)
    conv_out = (outer.astype(f32) * convolved).astype(bf16)

    forward_part = jnp.einsum("sihd,shde->sihe", rq, into_forward, preferred_element_type=f32)
    backward_part = jnp.einsum("sihd,shde->sihe", rq, into_backward, preferred_element_type=f32)
    mixed_heads = (
        local_part
        + jnp.exp(forward_cum).transpose(0, 2, 1)[..., None] * forward_part
        + jnp.exp(backward_cum).transpose(0, 2, 1)[..., None] * backward_part
    )
    scaled = mixed_heads * lax.rsqrt(
        jnp.mean(mixed_heads * mixed_heads, axis=-1, keepdims=True) + EPS
    )
    own_head_gain = lax.dynamic_slice_in_dim(head_gain, place * channels, channels)
    scaled = scaled.reshape(group, length, channels) * own_head_gain
    gate = rest[:, 3 * channels :].reshape(group, length, channels)
    ret_out = (jax.nn.silu(gate.astype(f32)) * scaled).astype(bf16)

    features = jnp.concatenate([conv_out, ret_out], axis=-1)
    features = features.reshape(group, 2, length // 2, 2 * channels)
    mine_rows, their_rows = pick(features, core, 1), pick(features, 1 - core, 1)
    half_out = out_weight.shape[1] // 2

    def partial(rows, ids, weight):
        picked = jnp.concatenate([rows[i] for i in ids], axis=0)
        return jnp.dot(picked, weight, preferred_element_type=f32)

    def chip_sum(ids, weight):
        theirs = cross(partial(their_rows, ids, weight).astype(bf16))
        total = partial(mine_rows, ids, weight) + theirs.astype(f32)
        return total.reshape(len(ids), length // 2, half_out)

    def scatter(weight, one, two):
        sent = swap(chip_sum((one, one ^ two), weight).astype(bf16), one)
        kept = chip_sum((0, two), weight) + sent.astype(f32)
        return kept[0] + swap(kept[1].astype(bf16), two).astype(f32)

    return jnp.concatenate(
        [
            scatter(out_weight[:, :half_out], 1, 2),
            scatter(out_weight[:, half_out:], 2, 1),
        ],
        axis=1,
    ).astype(bf16)


LANES = 128


def plan(*arrays):
    spans, cores = lax.axis_size("sp"), lax.axis_size("tp")
    group = arrays[2].shape[1] // LANES
    planes = spans // group
    fits = (
        cores == 2
        and group == 4
        and planes * group == spans
        and planes == 2 * cores
        and arrays[0].shape[1] == 2 * group * arrays[2].shape[0]
    )
    return plane_local(planes, group, arrays) if fits else local(*arrays)


def solution(mesh):
    return jax.shard_map(
        plan,
        mesh=mesh,
        in_specs=(
            P("sp", "tp"),
            P(),
            P("sp", "tp"),
            P("sp", "tp"),
            P("sp", "tp"),
            P("sp", "tp"),
            P("sp", "tp"),
            P("sp", "tp"),
            P("sp", "tp"),
            P(None, "tp"),
            P(None, "tp", "sp"),
            P("tp"),
            P("tp", "sp"),
            P("tp", "sp"),
        ),
        out_specs=P(("sp", "tp"), None),
        check_vma=False,
    )
```

```python
import jax
import functools
import jax.numpy as jnp
from jax import lax
from jax.experimental import pallas as pl
from jax.experimental.pallas import tpu as pltpu
from jax.sharding import PartitionSpec as P

HEAD_DIM = 64


EPS = 1e-06
THETA = 10000.0


def with_halo(shard, sides, width):
    for axis, dim in sides:
        size, length = (lax.axis_size(axis), shard.shape[dim])
        up = [(i, (i + 1) % size) for i in range(size - 1)]
        down = [(j, i) for i, j in up]
        last = lax.slice_in_dim(shard, length - width, length, axis=dim)
        first = lax.slice_in_dim(shard, 0, width, axis=dim)
        before = lax.ppermute(last, axis, up)
        after = lax.ppermute(first, axis, down)
        shard = jnp.concatenate([before, shard, after], axis=dim)
    return shard


def rotate(field_in, position_list):
    half_dim = field_in.shape[-1] // 2
    frequency = jnp.exp(
        -jnp.log(THETA) * jnp.arange(half_dim, dtype=jnp.float32) * (2.0 / field_in.shape[-1])
    )
    angles = position_list.astype(jnp.float32)[:, None, None] * frequency
    cosine = jnp.cos(angles)
    sine_part = jnp.sin(angles)
    leading = field_in[..., :half_dim]
    trailing = field_in[..., half_dim:]
    return jnp.concatenate(
        [leading * cosine - trailing * sine_part, leading * sine_part + trailing * cosine], axis=-1
    )


def conv_branch(outer_rows, inner_rows, conv_values, conv_taps):
    inner_value = (inner_rows.astype(jnp.float32) * conv_values.astype(jnp.float32)).astype(
        jnp.bfloat16
    )
    padded = with_halo(inner_value, (("sp", 0),), 1).astype(jnp.float32)
    convolved = conv_taps[0] * padded[:-2] + conv_taps[1] * padded[1:-1] + conv_taps[2] * padded[2:]
    return (outer_rows.astype(jnp.float32) * convolved).astype(jnp.bfloat16)


def span_parts(query_rows, key_rows, value_rows, log_rates):
    length = query_rows.shape[0]
    forward_cum = jnp.cumsum(log_rates[0], axis=-1)
    backward_cum = jnp.flip(jnp.cumsum(jnp.flip(log_rates[1], -1), axis=-1), -1)
    row_index = lax.broadcasted_iota(jnp.int32, (length, length), 0)
    col_index = lax.broadcasted_iota(jnp.int32, (length, length), 1)
    lower_part = (col_index <= row_index)[None]
    spread = jnp.where(
        lower_part,
        forward_cum[:, :, None] - forward_cum[:, None, :],
        backward_cum[:, :, None] - backward_cum[:, None, :],
    )
    scores = jnp.einsum("ihe,jhe->hij", query_rows, key_rows, preferred_element_type=jnp.float32)
    weighted = (scores * jnp.exp(spread)).astype(jnp.bfloat16)
    local_part = jnp.einsum(
        "hij,jhe->ihe", weighted, value_rows, preferred_element_type=jnp.float32
    )
    key_wide = key_rows.astype(jnp.float32)
    forward_keys = (key_wide * jnp.exp(forward_cum[:, -1:] - forward_cum).T[:, :, None]).astype(
        jnp.bfloat16
    )
    backward_keys = (key_wide * jnp.exp(backward_cum[:, :1] - backward_cum).T[:, :, None]).astype(
        jnp.bfloat16
    )
    forward_state = jnp.einsum(
        "jhd,jhe->hde", forward_keys, value_rows, preferred_element_type=jnp.float32
    )
    backward_state = jnp.einsum(
        "jhd,jhe->hde", backward_keys, value_rows, preferred_element_type=jnp.float32
    )
    return (local_part, forward_cum, backward_cum, forward_state, backward_state)


def retention_branch(query_rows, key_rows, value_rows, gate_rows, log_decay, head_gain, offsets):
    row_count = query_rows.shape[0]
    head_count = query_rows.shape[1] // HEAD_DIM
    shape_heads = (row_count, head_count, HEAD_DIM)
    rotated_query = rotate(query_rows.astype(jnp.float32).reshape(shape_heads), offsets).astype(
        jnp.bfloat16
    )
    rotated_key = (
        rotate(key_rows.astype(jnp.float32).reshape(shape_heads), offsets) * HEAD_DIM ** (-0.5)
    ).astype(jnp.bfloat16)
    local_part, forward_cum, backward_cum, forward_state, backward_state = span_parts(
        rotated_query, rotated_key, value_rows.reshape(shape_heads), log_decay
    )
    forward_total = forward_cum[:, -1]
    backward_total = backward_cum[:, 0]
    totals = lax.all_gather(
        jnp.stack([forward_total, backward_total])[None], "sp", axis=0, tiled=True
    )
    inclusive = jnp.cumsum(totals, axis=0)
    exclusive = inclusive - totals
    own_index = lax.axis_index("sp")
    own_inclusive = lax.dynamic_index_in_dim(inclusive, own_index, 0, keepdims=False)
    own_exclusive = lax.dynamic_index_in_dim(exclusive, own_index, 0, keepdims=False)
    pieces = (
        lax.all_gather(forward_state[None], "sp", axis=0, tiled=True),
        lax.all_gather(backward_state[None], "sp", axis=0, tiled=True),
    )
    piece_count = pieces[0].shape[0]
    span_index = lax.iota(jnp.int32, piece_count)
    forward_weight = jnp.where(
        (span_index < own_index)[:, None],
        jnp.exp(jnp.minimum(own_exclusive[0] - inclusive[:, 0], 0.0)),
        0.0,
    )
    backward_weight = jnp.where(
        (span_index > own_index)[:, None],
        jnp.exp(jnp.minimum(exclusive[:, 1] - own_inclusive[1], 0.0)),
        0.0,
    )
    into_forward = jnp.einsum(
        "nh,nhde->hde", forward_weight, pieces[0], precision=lax.Precision.HIGHEST
    )
    into_backward = jnp.einsum(
        "nh,nhde->hde", backward_weight, pieces[1], precision=lax.Precision.HIGHEST
    )
    forward_part = jnp.einsum(
        "ihd,hde->ihe",
        rotated_query,
        into_forward.astype(jnp.bfloat16),
        preferred_element_type=jnp.float32,
    )
    backward_part = jnp.einsum(
        "ihd,hde->ihe",
        rotated_query,
        into_backward.astype(jnp.bfloat16),
        preferred_element_type=jnp.float32,
    )
    mixed_heads = (
        local_part
        + jnp.exp(forward_cum).T[:, :, None] * forward_part
        + jnp.exp(backward_cum).T[:, :, None] * backward_part
    )
    scaled = mixed_heads * lax.rsqrt(
        jnp.mean(mixed_heads * mixed_heads, axis=-1, keepdims=True) + EPS
    )
    scaled = scaled * head_gain.reshape(head_count, HEAD_DIM)
    return (
        jax.nn.silu(gate_rows.astype(jnp.float32))
        * scaled.reshape(row_count, head_count * HEAD_DIM)
    ).astype(jnp.bfloat16)


def local(
    tokens,
    norm_gain,
    outer_gate,
    inner_gate,
    conv_input,
    query_proj,
    key_proj,
    value_proj,
    out_gate,
    conv_taps,
    log_decay,
    head_gain,
    conv_output,
    retention_output,
):
    whole = lax.all_gather(tokens, "tp", axis=1, tiled=True)
    wide = whole.astype(jnp.float32)
    normed = (
        wide * lax.rsqrt(jnp.mean(wide * wide, axis=-1, keepdims=True) + EPS) * norm_gain
    ).astype(jnp.bfloat16)
    row_count = normed.shape[0]
    offsets = lax.axis_index("sp") * row_count + lax.iota(jnp.int32, row_count)
    gathered = (
        lax.all_gather(outer_gate, "sp", axis=0, tiled=True),
        lax.all_gather(inner_gate, "sp", axis=0, tiled=True),
        lax.all_gather(conv_input, "sp", axis=0, tiled=True),
        lax.all_gather(query_proj, "sp", axis=0, tiled=True),
        lax.all_gather(key_proj, "sp", axis=0, tiled=True),
        lax.all_gather(value_proj, "sp", axis=0, tiled=True),
        lax.all_gather(out_gate, "sp", axis=0, tiled=True),
        lax.all_gather(conv_output, "sp", axis=1, tiled=True),
        lax.all_gather(retention_output, "sp", axis=1, tiled=True),
    )
    projected = [
        jnp.dot(normed, weight, preferred_element_type=jnp.float32).astype(jnp.bfloat16)
        for weight in gathered[:7]
    ]
    conv_out = conv_branch(projected[0], projected[1], projected[2], conv_taps)
    ret_out = retention_branch(
        projected[3], projected[4], projected[5], projected[6], log_decay, head_gain, offsets
    )
    conv_weight = gathered[7]
    ret_weight = gathered[8]
    return lax.psum_scatter(
        (
            jnp.dot(conv_out, conv_weight, preferred_element_type=jnp.float32)
            + jnp.dot(ret_out, ret_weight, preferred_element_type=jnp.float32)
        ).astype(jnp.bfloat16),
        "tp",
        scatter_dimension=0,
        tiled=True,
    )


def flipped(place, d):
    if d == 0:
        return place
    if d == 1:
        return place + 1 - 2 * lax.rem(place, 2)
    if d == 2:
        return place + 2 - 4 * lax.rem(lax.div(place, 2), 2)
    return 3 - place


def gather_kernel(
    planes, group, rows_ref, win_ref, wout_ref, rate_ref,
    x_ref, wi_ref, wo_ref, r_ref,
    near_send, near_recv, far_send, far_recv, tok_send, tok_recv, half_send, half_recv, own_sem,
):
    own, core = lax.axis_index("sp"), lax.axis_index("tp")
    place, plane = lax.rem(own, group), lax.div(own, group)
    base = plane * group
    half = rows_ref.shape[1]
    quarter = half // 2
    has_up, has_down = plane < planes - 1, plane > 0
    chips = [base + flipped(place, d) for d in range(group)]

    barrier = pltpu.get_barrier_semaphore()

    def greet(target):
        pl.semaphore_signal(
            barrier, inc=1, device_id=target, device_id_type=pl.DeviceIdType.MESH
        )

    for d in range(1, group):
        greet((chips[d], core))
    greet((own, 1 - core))
    pl.when(has_up)(lambda: greet((own + group, core)))
    pl.when(has_down)(lambda: greet((own - group, core)))
    pl.semaphore_wait(barrier, group + jnp.where(has_up, 1, 0) + jnp.where(has_down, 1, 0))

    def remote(source, target, send, recv, device):
        return pltpu.make_async_remote_copy(
            src_ref=source, dst_ref=target, send_sem=send, recv_sem=recv,
            device_id=device, device_id_type=pl.DeviceIdType.MESH,
        )

    def part(d, which):
        return x_ref.at[d, :, pl.ds(pl.multiple_of(core * half + which * quarter, 128), quarter)]

    def side(d):
        return x_ref.at[d, :, pl.ds(pl.multiple_of(core * half, 128), half)]

    kept = [
        pltpu.make_async_copy(win_ref.at[place], wi_ref.at[plane, place], own_sem.at[0]),
        pltpu.make_async_copy(wout_ref.at[place], wo_ref.at[plane, place], own_sem.at[1]),
        pltpu.make_async_copy(rate_ref.at[place], r_ref.at[0], own_sem.at[2]),
        pltpu.make_async_copy(rows_ref, side(0), own_sem.at[3]),
    ]
    for copy in kept:
        copy.start()

    near = []
    for kind, (source, target) in enumerate(((win_ref, wi_ref), (wout_ref, wo_ref), (rate_ref, r_ref))):
        for d in range(1, group):
            to = flipped(place, d)
            landing = target.at[d] if kind == 2 else target.at[plane, place]
            near.append(
                remote(source.at[to], landing, near_send.at[kind, d], near_recv.at[kind, d], (chips[d], core))
            )
    for copy in near[: group - 1]:
        copy.start()

    def pieces(which):
        return rows_ref.at[:, pl.ds(which * quarter, quarter)]

    tokens = {}

    def send_part(which, source, d_there, hop):
        tokens[(which, d_there)] = remote(
            source, part(d_there, which), tok_send.at[which, d_there], tok_recv.at[which, d_there],
            (chips[hop], core),
        )
        tokens[(which, d_there)].start()

    send_part(0, pieces(0), 1, 1)
    send_part(1, pieces(1), 2, 2)
    send_part(1, pieces(1), 1, 1)
    send_part(0, pieces(0), 2, 2)
    for copy in near[group - 1 :]:
        copy.start()
    partner = (own, 1 - core)
    halves = [remote(rows_ref, side(0), half_send.at[0], half_recv.at[0], partner)]
    halves[0].start()

    def far(kind, ref, direction, k, d):
        q = plane - k if direction == 0 else plane + k
        block = ref.at[q, flipped(place, d)]
        index = (kind, direction, k, d)
        target = own + group if direction == 0 else own - group
        return remote(block, block, far_send.at[index], far_recv.at[index], (target, core))

    def holds(direction, k):
        return plane - k >= 0 if direction == 0 else plane + k < planes

    def forwards(direction, k):
        return jnp.logical_and(holds(direction, k), has_up if direction == 0 else has_down)

    def landed(kind, ref, direction, k, d):
        q = plane - k if direction == 0 else plane + k
        block = ref.at[q, flipped(place, d)]
        index = (kind, direction, k - 1, d)
        remote(block, block, far_send.at[index], far_recv.at[index], (own, 1 - core)).wait_recv()

    def pass_on(kind, ref, k):
        for d in range(group):
            if k == 0:
                if d == 0:
                    kept[kind].wait()
                else:
                    near[kind * (group - 1) + d - 1].wait_recv()
            for direction in range(2):
                if k > 0:
                    pl.when(holds(direction, k))(
                        functools.partial(landed, kind, ref, direction, k, d)
                    )
                if k < planes - 1:
                    pl.when(forwards(direction, k))(
                        lambda direction=direction, d=d: far(kind, ref, direction, k, d).start()
                    )

    pass_on(0, wi_ref, 0)

    tokens[(0, 1)].wait_recv()
    send_part(0, part(1, 0), 3, 2)
    tokens[(1, 2)].wait_recv()
    send_part(1, part(2, 1), 3, 1)
    pass_on(1, wo_ref, 0)
    for which, d in ((1, 1), (0, 2), (0, 3), (1, 3)):
        tokens[(which, d)].wait_recv()
        if (which, d) in ((1, 1), (0, 2)):
            at = d
        elif which == 1:
            at = 3
        else:
            continue
        copy = remote(side(at), side(at), half_send.at[at], half_recv.at[at], partner)
        copy.start()
        halves.append(copy)

    for k in range(1, planes):
        pass_on(0, wi_ref, k)
        pass_on(1, wo_ref, k)

    for copy in kept[2:]:
        copy.wait()
    for copy in near:
        copy.wait_send()
    for copy in near[2 * (group - 1) :]:
        copy.wait_recv()
    for copy in tokens.values():
        copy.wait_send()
    for copy in halves:
        copy.wait()
    for kind, ref in enumerate((wi_ref, wo_ref)):
        for k in range(planes - 1):
            for d in range(group):
                for direction in range(2):
                    pl.when(forwards(direction, k))(
                        lambda kind=kind, ref=ref, direction=direction, k=k, d=d: far(
                            kind, ref, direction, k, d
                        ).wait_send()
                    )


def gather_all(planes, group, rows, weights_in, weights_out, rates):
    length, half = rows.shape
    dma = pltpu.SemaphoreType.DMA
    return pl.pallas_call(
        functools.partial(gather_kernel, planes, group),
        out_shape=(
            jax.ShapeDtypeStruct((group, length, 2 * half), rows.dtype),
            jax.ShapeDtypeStruct((planes,) + weights_in.shape, weights_in.dtype),
            jax.ShapeDtypeStruct((planes,) + weights_out.shape, weights_out.dtype),
            jax.ShapeDtypeStruct(rates.shape, rates.dtype),
        ),
        in_specs=[pl.BlockSpec(memory_space=pl.ANY)] * 4,
        out_specs=[pl.BlockSpec(memory_space=pl.ANY)] * 4,
        scratch_shapes=[
            dma((3, group)), dma((3, group)),
            dma((2, 2, planes, group)), dma((2, 2, planes, group)),
            dma((2, group)), dma((2, group)),
            dma((group,)), dma((group,)),
            dma((4,)),
        ],
        compiler_params=pltpu.CompilerParams(collective_id=0, has_side_effects=True),
    )(rows, weights_in, weights_out, rates)


def line_kernel(planes, group, f_ref, b_ref, of_ref, ob_ref, send, recv):
    own, core = lax.axis_index("sp"), lax.axis_index("tp")
    plane = lax.div(own, group)
    barrier = pltpu.get_barrier_semaphore()
    mesh_id = pl.DeviceIdType.MESH

    def greet(target):
        pl.semaphore_signal(barrier, inc=1, device_id=(target, core), device_id_type=mesh_id)

    moves = []
    for k in range(1, planes):
        ahead, behind = plane + k < planes, plane - k >= 0
        pl.when(ahead)(functools.partial(greet, own + k * group))
        pl.when(behind)(functools.partial(greet, own - k * group))
        forward = functools.partial(
            pltpu.make_async_remote_copy,
            src_ref=f_ref, dst_ref=of_ref.at[k - 1], send_sem=send.at[0, k], recv_sem=recv.at[0, k],
            device_id_type=mesh_id,
        )
        backward = functools.partial(
            pltpu.make_async_remote_copy,
            src_ref=b_ref, dst_ref=ob_ref.at[k - 1], send_sem=send.at[1, k], recv_sem=recv.at[1, k],
            device_id_type=mesh_id,
        )
        moves.append((forward, ahead, behind, own + k * group, own - k * group))
        moves.append((backward, behind, ahead, own - k * group, own + k * group))
    pl.semaphore_wait(barrier, planes - 1)
    for make, gives, _, target, _ in moves:
        pl.when(gives)(lambda make=make, target=target: make(device_id=(target, core)).start())
    for make, gives, takes, target, source in moves:
        pl.when(takes)(lambda make=make, source=source: make(device_id=(source, core)).wait_recv())
        pl.when(gives)(lambda make=make, target=target: make(device_id=(target, core)).wait_send())


def pass_line(planes, group, forward, backward):
    out = jax.ShapeDtypeStruct((planes - 1,) + forward.shape, forward.dtype)
    vmem = pl.BlockSpec(memory_space=pltpu.VMEM)
    return pl.pallas_call(
        functools.partial(line_kernel, planes, group),
        out_shape=(out, out),
        in_specs=[vmem] * 2,
        out_specs=[vmem] * 2,
        scratch_shapes=[pltpu.SemaphoreType.DMA((2, planes))] * 2,
        compiler_params=pltpu.CompilerParams(collective_id=1, has_side_effects=True),
    )(forward, backward)


def plane_local(planes, group, arrays):
    (
        tokens,
        norm_gain,
        outer_gate,
        inner_gate,
        conv_input,
        query_proj,
        key_proj,
        value_proj,
        out_gate,
        conv_taps,
        log_decay,
        head_gain,
        conv_output,
        retention_output,
    ) = arrays
    spans = planes * group
    own = lax.axis_index("sp")
    core = lax.axis_index("tp")
    place = lax.rem(own, group)
    plane = lax.div(own, group)
    length, half_width = tokens.shape
    width = half_width * 2
    channels = outer_gate.shape[1] // group
    heads = channels // HEAD_DIM
    f32, bf16 = jnp.float32, jnp.bfloat16

    def swap(x, d):
        return lax.ppermute(x, "sp", [(i, i ^ d) for i in range(spans)])

    def up(x, k=1):
        return lax.ppermute(x, "sp", [(i, i + k * group) for i in range(spans - k * group)])

    def down(x, k=1):
        return lax.ppermute(x, "sp", [(i + k * group, i) for i in range(spans - k * group)])

    def cross(x):
        return lax.ppermute(x, "tp", [(0, 1), (1, 0)])

    def pick(x, index, axis=0):
        return lax.dynamic_index_in_dim(x, index, axis, keepdims=False)

    def reorder(pieces):
        stacked = jnp.stack(pieces) if isinstance(pieces, (list, tuple)) else pieces
        return jnp.stack([pick(stacked, jnp.bitwise_xor(place, t)) for t in range(group)])

    wide = tokens.astype(f32)
    square_sum = jnp.sum(wide * wide, axis=-1).reshape(-1, 128)
    square_sum = (square_sum + cross(square_sum)).reshape(length, 1)
    own_gain = lax.dynamic_slice_in_dim(norm_gain, core * half_width, half_width)
    normed = (wide * lax.rsqrt(square_sum / width + EPS) * own_gain).astype(bf16)

    rows_in = outer_gate.shape[0]
    weights_in = jnp.stack(
        [
            w.reshape(rows_in, group, channels)
            for w in (key_proj, query_proj, value_proj, inner_gate, conv_input, outer_gate, out_gate)
        ],
        axis=2,
    ).reshape(rows_in, group, 7 * channels).transpose(1, 0, 2)
    out_cols = conv_output.shape[1]
    weights_out = jnp.concatenate(
        [w.reshape(group, channels, out_cols) for w in (conv_output, retention_output)], axis=1
    )
    own_rates = log_decay.reshape(2, group, heads, length).transpose(1, 0, 2, 3)
    rows_all, win_all, wout_all, rates = gather_all(
        planes, group, normed, weights_in, weights_out, own_rates.reshape(group, 2 * heads, length)
    )
    rates = rates.reshape(group, 2, heads, length)
    projected = jnp.dot(
        rows_all.reshape(group * length, width),
        win_all.reshape(width, 7 * channels),
        preferred_element_type=f32,
    ).astype(bf16)
    out_weight = wout_all.transpose(2, 0, 1, 3).reshape(2 * channels, width)

    span_ids = plane * group + jnp.bitwise_xor(place, lax.iota(jnp.int32, group))
    positions = (span_ids[:, None] * length + lax.iota(jnp.int32, length)).reshape(-1)
    half_dim = HEAD_DIM // 2
    frequency = jnp.exp(
        -jnp.log(THETA) * jnp.arange(half_dim, dtype=f32) * (2.0 / HEAD_DIM)
    )
    angles = positions.astype(f32)[:, None] * frequency
    cosine, sine = lax.optimization_barrier((jnp.cos(angles), jnp.sin(angles)))
    cosine, sine = cosine[:, None, :], sine[:, None, :]

    def turned(x):
        x = x.astype(f32).reshape(group * length, heads, HEAD_DIM)
        a, b = x[..., :half_dim], x[..., half_dim:]
        return jnp.concatenate([a * cosine - b * sine, a * sine + b * cosine], axis=-1)

    shape_heads = (group, length, heads, HEAD_DIM)
    kqv, rest = projected[:, : 3 * channels], projected[:, 3 * channels :]
    rk = (turned(kqv[:, :channels]) * HEAD_DIM ** (-0.5)).astype(bf16).reshape(shape_heads)
    rq = turned(kqv[:, channels : 2 * channels]).astype(bf16).reshape(shape_heads)
    value = kqv[:, 2 * channels :].reshape(shape_heads)
    local_part, forward_cum, backward_cum, forward_state, backward_state = jax.vmap(span_parts)(
        rq, rk, value, rates
    )
    forward_total = reorder(forward_cum[:, :, -1])
    backward_total = reorder(backward_cum[:, :, 0])
    forward_state = reorder(forward_state)
    backward_state = reorder(backward_state)

    inner_value = (
        rest[:, :channels].astype(f32) * rest[:, channels : 2 * channels].astype(f32)
    ).astype(bf16).reshape(group, length, channels)
    lasts = reorder(inner_value[:, -1:])
    firsts = reorder(inner_value[:, :1])

    def gather_up(states, totals, edge):
        running = jnp.zeros_like(states[0])
        passed = jnp.zeros_like(totals[0])
        inside, reach = [], []
        for state, total in zip(states, totals):
            inside.append(running)
            reach.append(passed)
            running = jnp.exp(total)[:, None, None] * running + state
            passed = passed + total
        body = running.reshape(-1, channels)
        row = jnp.pad(passed, (0, channels - heads))[None]
        rows = [body, row, edge.astype(f32)]
        return inside, reach, jnp.pad(jnp.concatenate(rows, axis=0), ((0, 6), (0, 0)))

    def finish_carry(inside, reach, packs, exists):
        packs = [jnp.where(e, p, 0.0) for e, p in zip(exists, packs)]
        count = heads * HEAD_DIM * HEAD_DIM // channels
        incoming, between = jnp.zeros_like(inside[0]), jnp.zeros_like(reach[0])
        for pack in packs:
            state = pack[:count].reshape(heads, HEAD_DIM, HEAD_DIM)
            incoming = incoming + jnp.exp(between)[:, None, None] * state
            between = between + pack[count, :heads]
        into = [a + jnp.exp(b)[:, None, None] * incoming for a, b in zip(inside, reach)]
        return into, packs[0][count + 1][None, None].astype(bf16)

    forward_in, forward_reach, forward_pack = gather_up(
        list(forward_state), list(forward_total), lasts[-1]
    )
    backward_in, backward_reach, backward_pack = gather_up(
        list(backward_state)[::-1], list(backward_total)[::-1], firsts[0]
    )
    forward_got, backward_got = pass_line(planes, group, forward_pack, backward_pack)
    steps = range(1, planes)
    into_forward, edge_before = finish_carry(
        forward_in, forward_reach, list(forward_got), [plane - k >= 0 for k in steps]
    )
    into_backward, edge_after = finish_carry(
        backward_in, backward_reach, list(backward_got), [plane + k < planes for k in steps]
    )
    into_forward = reorder(into_forward).astype(bf16)
    into_backward = reorder(into_backward[::-1]).astype(bf16)
    before = reorder(jnp.concatenate([edge_before, lasts[:-1]], axis=0))
    after = reorder(jnp.concatenate([firsts[1:], edge_after], axis=0))
    taps = lax.dynamic_slice_in_dim(conv_taps, place * channels, channels, axis=1)
    padded = jnp.concatenate([before, inner_value, after], axis=1).astype(f32)
    convolved = taps[0] * padded[:, :-2] + taps[1] * padded[:, 1:-1] + taps[2] * padded[:, 2:]
    outer = rest[:, 2 * channels : 3 * channels].reshape(group, length, channels)
    conv_out = (outer.astype(f32) * convolved).astype(bf16)

    forward_part = jnp.einsum("sihd,shde->sihe", rq, into_forward, preferred_element_type=f32)
    backward_part = jnp.einsum("sihd,shde->sihe", rq, into_backward, preferred_element_type=f32)
    mixed_heads = (
        local_part
        + jnp.exp(forward_cum).transpose(0, 2, 1)[..., None] * forward_part
        + jnp.exp(backward_cum).transpose(0, 2, 1)[..., None] * backward_part
    )
    scaled = mixed_heads * lax.rsqrt(
        jnp.mean(mixed_heads * mixed_heads, axis=-1, keepdims=True) + EPS
    )
    own_head_gain = lax.dynamic_slice_in_dim(head_gain, place * channels, channels)
    scaled = scaled.reshape(group, length, channels) * own_head_gain
    gate = rest[:, 3 * channels :].reshape(group, length, channels)
    ret_out = (jax.nn.silu(gate.astype(f32)) * scaled).astype(bf16)

    features = jnp.concatenate([conv_out, ret_out], axis=-1)
    features = features.reshape(group, 2, length // 2, 2 * channels)
    mine_rows, their_rows = pick(features, core, 1), pick(features, 1 - core, 1)
    half_out = out_weight.shape[1] // 2

    def partial(rows, ids, weight):
        picked = jnp.concatenate([rows[i] for i in ids], axis=0)
        return jnp.dot(picked, weight, preferred_element_type=f32)

    def chip_sum(ids, weight):
        theirs = cross(partial(their_rows, ids, weight).astype(bf16))
        total = partial(mine_rows, ids, weight) + theirs.astype(f32)
        return total.reshape(len(ids), length // 2, half_out)

    def scatter(weight, one, two):
        sent = swap(chip_sum((one, one ^ two), weight).astype(bf16), one)
        kept = chip_sum((0, two), weight) + sent.astype(f32)
        return kept[0] + swap(kept[1].astype(bf16), two).astype(f32)

    return jnp.concatenate(
        [
            scatter(out_weight[:, :half_out], 1, 2),
            scatter(out_weight[:, half_out:], 2, 1),
        ],
        axis=1,
    ).astype(bf16)


LANES = 128


def plan(*arrays):
    spans, cores = lax.axis_size("sp"), lax.axis_size("tp")
    group = arrays[2].shape[1] // LANES
    planes = spans // group
    fits = (
        cores == 2
        and group == 4
        and planes * group == spans
        and planes == 2 * cores
        and arrays[0].shape[1] == 2 * group * arrays[2].shape[0]
    )
    return plane_local(planes, group, arrays) if fits else local(*arrays)


def solution(mesh):
    return jax.shard_map(
        plan,
        mesh=mesh,
        in_specs=(
            P("sp", "tp"),
            P(),
            P("sp", "tp"),
            P("sp", "tp"),
            P("sp", "tp"),
            P("sp", "tp"),
            P("sp", "tp"),
            P("sp", "tp"),
            P("sp", "tp"),
            P(None, "tp"),
            P(None, "tp", "sp"),
            P("tp"),
            P("tp", "sp"),
            P("tp", "sp"),
        ),
        out_specs=P(("sp", "tp"), None),
        check_vma=False,
    )
```
